256 devices in a mesh: ep: 16 (over y, x), tp: 16 (over z, core).
Axes of the slice: x: 4, y: 4, z: 8, core: 2. Of those that a mesh axis runs over, the one named last changes fastest.
Arguments:
- tokens: bfloat16 [256, 4096], P('ep'), may hold values from -6 to 6
- attn_gain: float32 [4096], replicated, may hold values from 0.1 to 1.9
- w_query: bfloat16 [4096, 2048], P('ep', 'tp'), may hold values from -0.15625 to 0.15625
- w_key: bfloat16 [4096, 2048], P('ep', 'tp'), may hold values from -0.09375 to 0.09375
- w_value: bfloat16 [4096, 2048], P('ep', 'tp'), may hold values from -0.09375 to 0.09375
- mix_lambda: float32 [16], P('tp'), may hold values from 0.3 to 0.8
- head_gain: float32 [128], replicated, may hold values from 0.1 to 1.9
- w_output: bfloat16 [2048, 4096], P('tp'), may hold values from -0.125 to 0.125
- cache_keys: bfloat16 [256, 1024, 2048], P('ep', None, 'tp'), may hold values from -180 to 180
- cache_value: bfloat16 [256, 1024, 2048], P('ep', None, 'tp'), may hold values from -6 to 6
- lengths: int32 [256], P('ep'), may hold values from 1 to 1024
- moe_gain: float32 [4096], replicated, may hold values from 0.1 to 1.9
- group_ids: int32 [256], P('ep'), may hold values from 0 to 7, as said below
- member_ids: int32 [256, 2], P('ep'), may hold values from 0 to 1, as said below
- group_gate: float32 [256], P('ep'), may hold values from 0.3 to 1
- member_logits: float32 [256, 2], P('ep'), may hold values from -4 to 4
- w_exp_gate: bfloat16 [16, 4096, 2048], P('ep', None, 'tp'), may hold values from -0.09375 to 0.09375
- w_exp_up: bfloat16 [16, 4096, 2048], P('ep', None, 'tp'), may hold values from -0.09375 to 0.09375
- w_exp_down: bfloat16 [16, 2048, 4096], P('ep', 'tp'), may hold values from -0.125 to 0.125
Outputs:
- mixed: bfloat16 [256, 4096], P('ep', 'tp')
- fresh_keys: bfloat16 [256, 2048], P('ep', 'tp')
- fresh_value: bfloat16 [256, 2048], P('ep', 'tp')
The draws below stay inside these ranges and needn't reach their ends.
Inputs may be any that keep to these rules, and one draw needn't show every extreme that they name: `group_ids`: each index of ep holds 16 consecutive tokens, of which every group gets the same number. A token's 2 members differ, and every expert group_ids * 2 + member_ids receives exactly 2 of the token-expert pairs of each index of ep.
All inputs are finite; a program needn't handle non-finite values.
Results may differ from the reference program's by a relative error of at most 0.015.
The reference program's roundings to bfloat16 on the way count: a program that leaves them out, or rounds other values in their place, can miss the bound.
Values may be sent and summed in bfloat16 or wider, within the bound.
A program may use at most 64 MiB of HBM per device.

```python
import jax
import jax.numpy as jnp
from jax import lax

D = 4096
HEADS = 16
DH = 64
FF = 2048
EPG = 2
TOPK = 2
SEQ_DEV = 16
CACHE = 1024
EXPERTS = 16
GROUPS = 8
BATCH = 256
N_EP = 16
N_TP = 16


def routing_tables(key):
    perm_key, start_key, shift_key = jax.random.split(jax.random.fold_in(key, 11), 3)
    perms = jax.vmap(lambda sub: jax.random.permutation(sub, SEQ_DEV))(jax.random.split(perm_key, N_EP))
    starts = jax.random.randint(start_key, (N_EP, GROUPS), 0, EPG)
    shifts = jax.random.randint(shift_key, (N_EP, GROUPS), 1, EPG)
    group = perms % GROUPS
    inside = perms // GROUPS
    start_row = jnp.take_along_axis(starts, group, axis=1)
    shift_row = jnp.take_along_axis(shifts, group, axis=1)
    first = (start_row + inside) % EPG
    second = (start_row + inside + shift_row) % EPG
    members = jnp.stack([first, second], axis=-1)
    return (group.reshape(BATCH).astype(jnp.int32), members.reshape(BATCH, TOPK).astype(jnp.int32))


def draw_group_ids(key, part):
    group, members = routing_tables(key)
    return group


def draw_member_ids(key, part):
    group, members = routing_tables(key)
    return members


def draw_cache_keys(key, part):
    base_key = jax.random.fold_in(jax.random.fold_in(key, 21), 0)
    base = jax.random.truncated_normal(base_key, -6.0, 6.0, (BATCH, CACHE, HEADS * 2 * DH), jnp.float32)
    return base.astype(jnp.bfloat16)


def touch_ends(entries, key, least, top_value):
    place = [jax.random.randint(jax.random.fold_in(key, axis), (), 0, length) for axis, length in enumerate(entries.shape)]
    main_axis = entries.shape.index(max(entries.shape))
    next_to = place[:main_axis] + [(place[main_axis] + 1) % entries.shape[main_axis]] + place[main_axis + 1:]
    return entries.at[tuple(place)].set(least).at[tuple(next_to)].set(top_value)


def block_levels(key, dims, cuts, smallest, largest):
    loudness, own = 1.0, jax.random.fold_in(key, 6)
    for dim, blocks in cuts:
        draws = jnp.exp(jax.random.uniform(jax.random.fold_in(own, dim), (blocks,), jnp.float32, smallest / len(cuts), largest / len(cuts)))
        loudness = loudness * jnp.repeat(draws, dims[dim] // blocks).reshape([-1 if axis == dim else 1 for axis in range(len(dims))])
    return loudness


def gaussian(rng, dims, width, most, shards=(), held_as=jnp.bfloat16):
    level = block_levels(rng, dims, shards, -0.22, 0.18) if shards else 1.0
    values = jax.random.normal(rng, dims, jnp.float32) * width * level
    return jnp.minimum(jnp.maximum(values, -most), most).astype(held_as)


def setup_inputs(seed: int = 0) -> dict:
    key_of = jax.random.split(jax.random.key(seed), 20)
    return {
        "tokens": gaussian(key_of[0], (BATCH, D), 1.0, 6.0, ((0, 16),)),
        "attn_gain": jnp.clip(1.0 + 0.18 * jax.random.normal(key_of[1], (D,), jnp.float32), 0.1, 1.9),
        "w_query": gaussian(key_of[2], (D, HEADS * 2 * DH), (D // 3) ** -0.5, 0.15625, ((0, 16), (1, 16))),
        "w_key": gaussian(key_of[3], (D, HEADS * 2 * DH), D ** -0.5, 0.09375, ((0, 16), (1, 16))),
        "w_value": gaussian(key_of[4], (D, HEADS * 2 * DH), D ** -0.5, 0.09375, ((0, 16), (1, 16))),
        "mix_lambda": jnp.clip(0.3 + 0.5 * jax.random.uniform(key_of[5], (HEADS,), jnp.float32) ** block_levels(key_of[5], (HEADS,), ((0, 16),), -0.2, 0.2), 0.3, 0.8),
        "head_gain": jnp.clip(1.0 + 0.18 * jax.random.normal(key_of[6], (2 * DH,), jnp.float32), 0.1, 1.9),
        "w_output": gaussian(key_of[7], (HEADS * 2 * DH, D), (HEADS * 2 * DH) ** -0.5, 0.125, ((0, 16),)),
        "cache_keys": draw_cache_keys(jax.random.fold_in(key_of[19], 71), 0),
        "cache_value": gaussian(key_of[9], (BATCH, CACHE, HEADS * 2 * DH), 1.0, 6.0, ((0, 16), (2, 16))),
        "lengths": touch_ends(jax.random.randint(key_of[10], (BATCH,), 1, CACHE + 1), jax.random.fold_in(key_of[10], 1), 1, CACHE).astype(jnp.int32),
        "moe_gain": jnp.clip(1.0 + 0.18 * jax.random.normal(key_of[11], (D,), jnp.float32), 0.1, 1.9),
        "group_ids": draw_group_ids(jax.random.fold_in(key_of[19], 71), 0),
        "member_ids": draw_member_ids(jax.random.fold_in(key_of[19], 71), 0),
        "group_gate": jnp.clip(0.3 + 0.7 * jax.random.uniform(key_of[14], (BATCH,), jnp.float32) ** block_levels(key_of[14], (BATCH,), ((0, 16),), -0.2, 0.2), 0.3, 1.0),
        "member_logits": gaussian(key_of[15], (BATCH, TOPK), 1.0, 4.0, ((0, 16),), jnp.float32),
        "w_exp_gate": gaussian(key_of[16], (EXPERTS, D, FF), D ** -0.5, 0.09375, ((0, 16), (2, 16))),
        "w_exp_up": gaussian(key_of[17], (EXPERTS, D, FF), D ** -0.5, 0.09375, ((0, 16), (2, 16))),
        "w_exp_down": gaussian(key_of[18], (EXPERTS, FF, D), FF ** -0.5, 0.125, ((0, 16), (1, 16))),
    }


EPS = 1e-06

def rms_scale(values, gain):
    return values * lax.rsqrt(lax.optimization_barrier(jnp.mean(values * values, axis=-1, keepdims=True)) + EPS) * gain

def reference(tokens, attn_gain, w_query, w_key, w_value, mix_lambda, head_gain, w_output, cache_keys, cache_value, lengths, moe_gain, group_ids, member_ids, group_gate, member_logits, w_exp_gate, w_exp_up, w_exp_down):
    resid_in = tokens.astype(jnp.float32)
    normed = rms_scale(resid_in, attn_gain).astype(jnp.bfloat16)

    def project(weight):
        return jnp.dot(normed, weight, preferred_element_type=jnp.float32).astype(jnp.bfloat16)
    query = project(w_query)
    fresh_keys = project(w_key)
    fresh_val = project(w_value)
    head_index = jnp.arange(HEADS).astype(jnp.float32)
    slopes = 2.0 ** (-8.0 * (head_index + 1.0) / HEADS)
    scale = DH ** (-0.5)
    lam = mix_lambda.astype(jnp.float32)

    def block(args):
        qry, knew, vnew, ckeys, cval, lens = args
        count = qry.shape[0]
        positions = jnp.arange(CACHE)
        dist = (lens[:, None] - positions[None, :]).astype(jnp.float32)
        valid = positions[None, :] < lens[:, None]
        qf = qry.reshape(count, HEADS, 2, DH).astype(jnp.float32)
        keys = ckeys.reshape(count, CACHE, HEADS, 2, DH).astype(jnp.float32)
        fresh = knew.reshape(count, HEADS, 2, DH).astype(jnp.float32)
        old = jnp.einsum('shcd,slhcd->cshl', qf, keys, precision=lax.Precision.HIGHEST) * scale
        old = old - slopes[None, None, :, None] * dist[None, :, None, :]
        old = jnp.where(valid[None, :, None, :], old, -jnp.inf)
        new = jnp.moveaxis(lax.optimization_barrier(jnp.sum(qf * fresh, axis=-1)) * scale, 2, 0)
        full = jnp.concatenate([old, new[..., None]], axis=-1)
        maps = jax.nn.softmax(full, axis=-1)
        weights = (maps[0] - lam[None, :, None] * maps[1]).astype(jnp.bfloat16)
        values = cval.reshape(count, CACHE, HEADS, 2 * DH).astype(jnp.float32)
        wide = weights.astype(jnp.float32)
        head_mix = jnp.einsum('shl,slhe->she', wide[..., :CACHE], values, precision=lax.Precision.HIGHEST)
        head_mix = head_mix + wide[..., CACHE][..., None] * vnew.reshape(count, HEADS, 2 * DH).astype(jnp.float32)
        head_out = rms_scale(head_mix, head_gain).astype(jnp.bfloat16)
        return head_out.reshape(count, HEADS * 2 * DH)

    def split(array):
        return array.reshape((N_EP, SEQ_DEV) + array.shape[1:])
    pieces = (split(query), split(fresh_keys), split(fresh_val), split(cache_keys), split(cache_value), split(lengths))
    head_out = lax.map(block, pieces).reshape(BATCH, HEADS * 2 * DH)
    group = HEADS * 2 * DH // N_TP
    attn_sum = jnp.zeros((BATCH, D), jnp.float32)
    for index in range(N_TP):
        term = jnp.dot(head_out[:, index * group:(index + 1) * group], w_output[index * group:(index + 1) * group], preferred_element_type=jnp.float32).astype(jnp.bfloat16)
        attn_sum = attn_sum + lax.optimization_barrier(term).astype(jnp.float32)
    resid = resid_in + attn_sum
    moe_in = rms_scale(resid, moe_gain).astype(jnp.bfloat16)
    expert_ids = group_ids[:, None] * EPG + member_ids
    route_weight = jax.nn.softmax(member_logits.astype(jnp.float32), axis=-1) * group_gate[:, None]

    def step(total, args):
        gate_w, up_w, down_w, index = args
        gate = jnp.dot(moe_in, gate_w, preferred_element_type=jnp.float32)
        upper = jnp.dot(moe_in, up_w, preferred_element_type=jnp.float32)
        hidden = (jax.nn.silu(gate) * upper).astype(jnp.bfloat16)
        result = jnp.dot(hidden, down_w, preferred_element_type=jnp.float32).astype(jnp.bfloat16)
        share = lax.optimization_barrier(jnp.sum(jnp.where(expert_ids == index, route_weight, 0.0), axis=1))
        return (total + share[:, None] * lax.optimization_barrier(result).astype(jnp.float32), None)
    routed, _ = lax.scan(step, jnp.zeros((BATCH, D), jnp.float32), (w_exp_gate, w_exp_up, w_exp_down, jnp.arange(EXPERTS).astype(jnp.int32)))
    mixed = (resid + routed).astype(jnp.bfloat16)
    return (mixed, fresh_keys, fresh_val)
```

```python
import functools

import jax
import jax.numpy as jnp
from jax import lax
from jax.experimental import pallas as pl
from jax.experimental.pallas import tpu as pltpu
from jax.sharding import PartitionSpec as P

EPG = 2
EPS = 1e-06
MESH = pl.DeviceIdType.MESH
HIGHEST = lax.Precision.HIGHEST
F32 = jnp.float32
BF16 = jnp.bfloat16
NT = (((1,), (1,)), ((), ()))


def iota(shape, dim):
    return lax.broadcasted_iota(jnp.int32, shape, dim)


def exact_dot(a, b, dims=(((1,), (0,)), ((), ()))):
    return lax.dot_general(a, b, dims, precision=HIGHEST, preferred_element_type=F32)


def layer_kernel(
    n,
    tokens_h,
    attn_gain_h,
    wq_h,
    wk_h,
    wv_h,
    lam_ref,
    head_gain_h,
    wo_h,
    keys_h,
    vals_h,
    lengths_ref,
    moe_gain_h,
    groups_ref,
    members_ref,
    gates_ref,
    logits_ref,
    wg_h,
    wu_h,
    wd_h,
    mixed_ref,
    fresh_k_ref,
    fresh_v_ref,
    tokens,
    attn_gain,
    wqkv,
    head_gain,
    wo,
    keys,
    vals,
    moe_gain,
    wgu,
    wd,
    rows_s,
    send_a,
    recv_a,
    send_b,
    recv_b,
    send_c,
    recv_c,
    send_e,
    recv_e,
    send_f,
    recv_f,
    send_s,
    recv_s,
    send_g,
    recv_g,
    send_h,
    recv_h,
    load_sem,
    ss,
    rs,
):
    ep = lax.axis_index("ep")
    tp = lax.axis_index("tp")
    width = tokens_h.shape[1]
    cols = width // n
    seqs = tokens_h.shape[0]
    hd = wq_h.shape[1]
    half = hd // 2
    cache = keys_h.shape[1]

    loads = [
        (tokens_h, tokens),
        (attn_gain_h, attn_gain),
        (wq_h, wqkv.at[:, pl.ds(0, hd)]),
        (wk_h, wqkv.at[:, pl.ds(hd, hd)]),
        (wv_h, wqkv.at[:, pl.ds(2 * hd, hd)]),
        (keys_h, keys),
        (vals_h, vals),
        (head_gain_h, head_gain),
        (wo_h, wo),
        (moe_gain_h, moe_gain),
        (wg_h.at[0], wgu.at[:, pl.ds(0, hd)]),
        (wu_h.at[0], wgu.at[:, pl.ds(hd, hd)]),
        (wd_h.at[0], wd),
    ]
    copies = [pltpu.make_async_copy(s, d, load_sem.at[i]) for i, (s, d) in enumerate(loads)]
    for copy in copies:
        copy.start()

    barrier = pltpu.get_barrier_semaphore()

    def greet(d, carry):
        pl.semaphore_signal(barrier, inc=1, device_id=(lax.rem(ep + d, n), tp), device_id_type=MESH)
        pl.semaphore_signal(barrier, inc=1, device_id=(ep, lax.rem(tp + d, n)), device_id_type=MESH)
        return carry

    lax.fori_loop(1, n, greet, 0)

    def block(ref, i, tiles):
        return ref.at[pl.ds(pl.multiple_of(i * 8, 8), 8), :] if tiles else ref.at[i]

    def exchange(phase, send, recv, over_ep, whole=False, tiles=False):
        me = ep if over_ep else tp

        def descriptor(d, incoming):
            peer = lax.rem(me + d, n)
            slot = peer if incoming else me
            target = (peer, tp) if over_ep else (ep, peer)
            return pltpu.make_async_remote_copy(
                src_ref=send if whole else block(send, peer, tiles),
                dst_ref=block(recv, slot, tiles),
                send_sem=ss.at[phase, peer],
                recv_sem=rs.at[phase, slot],
                device_id=target,
                device_id_type=MESH,
            )

        def start(d, carry):
            descriptor(d, False).start()
            return carry

        def arrived(d):
            descriptor(d, True).wait_recv()

        def sent(d, carry):
            descriptor(d, False).wait_send()
            return carry

        return start, arrived, sent

    def wait_all(arrived):
        def body(d, carry):
            arrived(d)
            return carry

        lax.fori_loop(1, n, body, 0)

    a_start, a_arrived, a_sent = exchange(0, send_a, recv_a, True)
    b_start, b_arrived, b_sent = exchange(1, send_b, recv_b, True)
    c_start, c_arrived, c_sent = exchange(2, send_c, recv_c, False)
    e_start, e_arrived, e_sent = exchange(3, send_e, recv_e, True, tiles=True)
    f_start, f_arrived, f_sent = exchange(4, send_f, recv_f, False, True)
    s_start, s_arrived, s_sent = exchange(5, send_s, recv_s, False, True)
    g_start, g_arrived, g_sent = exchange(6, send_g, recv_g, False)
    h_start, h_arrived, h_sent = exchange(7, send_h, recv_h, True, tiles=True)

    copies[0].wait()
    copies[1].wait()
    x = tokens[...].astype(F32)
    normed = x * lax.rsqrt(jnp.mean(x * x, axis=-1, keepdims=True) + EPS) * attn_gain[...]
    normed = normed.astype(BF16)
    for i in range(n):
        send_a[i] = normed[:, i * cols : (i + 1) * cols]
    recv_a[ep] = send_a[ep]
    pl.semaphore_wait(barrier, 2 * (n - 1))
    lax.fori_loop(1, n, a_start, 0)

    rows_s[...] = jnp.zeros_like(rows_s)
    rows_s[0:1, 0:seqs] = lengths_ref[...].astype(F32)
    rows_s[1:2, 0:seqs] = groups_ref[...].astype(F32)
    rows_s[2:4, 0:seqs] = members_ref[...].astype(F32)
    rows_s[4:5, 0:seqs] = gates_ref[...]
    rows_s[5:7, 0:seqs] = logits_ref[...]
    rows = rows_s[...][:, 0:seqs]
    eye = (iota((seqs, seqs), 0) == iota((seqs, seqs), 1)).astype(F32)
    columns = exact_dot(eye, rows, NT)
    id0_row = rows[1:2] * EPG + rows[2:3]
    id1_row = rows[1:2] * EPG + rows[3:4]
    id0_col = columns[:, 1:2] * EPG + columns[:, 2:3]
    id1_col = columns[:, 1:2] * EPG + columns[:, 3:4]
    logit_max = jnp.maximum(columns[:, 5:6], columns[:, 6:7])
    exp0 = jnp.exp(columns[:, 5:6] - logit_max)
    exp1 = jnp.exp(columns[:, 6:7] - logit_max)
    exp_sum = exp0 + exp1
    share0 = exp0 / exp_sum * columns[:, 4:5]
    share1 = exp1 / exp_sum * columns[:, 4:5]
    tall = 8 * n
    tall_row = iota((tall, seqs), 0)
    tall_expert = (tall_row // 8).astype(F32)
    tall_kind = tall_row % 8
    tall_rank = jnp.where((tall_kind == 2) | (tall_kind == 3) | (tall_kind == 5), 1.0, 0.0)
    chosen = ((id0_row == tall_expert) | (id1_row == tall_expert)).astype(F32)
    before = (iota((seqs, seqs), 0) < iota((seqs, seqs), 1)).astype(F32)
    rank = exact_dot(chosen, before)
    dispatch = jnp.where((rank == tall_rank) & (tall_kind < 6), chosen, 0.0)
    wide_col = iota((seqs, tall), 1)
    wide_expert = (wide_col // 8).astype(F32)
    wide_kind = wide_col % 8
    wide_rank = jnp.where(wide_kind >= 2, 1.0, 0.0)
    hit0 = (id0_col == wide_expert).astype(F32)
    hit1 = (id1_col == wide_expert).astype(F32)
    after = (iota((seqs, seqs), 1) < iota((seqs, seqs), 0)).astype(F32)
    wide_ranks = exact_dot(after, hit0 + hit1)
    combine = jnp.where((wide_ranks == wide_rank) & (wide_kind < 4), hit0 * share0 + hit1 * share1, 0.0)

    wait_all(a_arrived)
    for i in (2, 3, 4):
        copies[i].wait()
    everyone = recv_a[...].reshape(n * seqs, cols)
    partial = jnp.dot(everyone, wqkv[...], preferred_element_type=F32)
    send_b[...] = partial.reshape(n, seqs, 3 * hd)
    recv_b[ep] = send_b[ep]
    lax.fori_loop(1, n, b_start, 0)
    wait_all(b_arrived)
    projected = jnp.sum(recv_b[...], axis=0).astype(BF16)
    query = projected[:, 0:hd]
    fresh_k = projected[:, hd : 2 * hd]
    fresh_v = projected[:, 2 * hd : 3 * hd]
    fresh_k_ref[...] = fresh_k
    fresh_v_ref[...] = fresh_v

    total_heads = n
    slope = jnp.float32(0.0)
    for h in range(total_heads):
        slope = jnp.where(tp == h, jnp.float32(2.0 ** (-8.0 * (h + 1.0) / total_heads)), slope)
    scale = half ** (-0.5)
    both = 2 * seqs
    q2 = jnp.concatenate([query, query], axis=0).astype(F32)
    k2 = jnp.concatenate([fresh_k, fresh_k], axis=0).astype(F32)
    own_map = (iota((both, hd), 0) // seqs) == (iota((both, hd), 1) // half)
    q2 = jnp.where(own_map, q2, 0.0)
    new = jnp.sum(q2 * k2, axis=-1, keepdims=True) * scale
    q4 = jnp.concatenate([q2, q2], axis=1)
    q4_seq = iota((both, 2 * hd), 0) % seqs
    q4_side = iota((both, 2 * hd), 1) // hd
    copies[5].wait()

    def score_step(p, acc):
        lhs = jnp.where(q4_seq == 2 * p + q4_side, q4, 0.0).astype(BF16)
        rhs = jnp.concatenate([keys[2 * p], keys[2 * p + 1]], axis=1)
        return acc + lax.dot_general(lhs, rhs, NT, preferred_element_type=F32)

    old = lax.fori_loop(0, seqs // 2, score_step, jnp.zeros((both, cache), F32)) * scale
    count = jnp.concatenate([columns[:, 0:1], columns[:, 0:1]], axis=0)
    place = iota((both, cache), 1).astype(F32)
    old = jnp.where(place < count, old - slope * (count - place), -jnp.inf)
    top = jnp.maximum(jnp.max(old, axis=-1, keepdims=True), new)
    e_old = jnp.exp(old - top)
    e_new = jnp.exp(new - top)
    norm = jnp.sum(e_old, axis=-1, keepdims=True) + e_new
    m_old = e_old / norm
    m_new = e_new / norm
    lam = lam_ref[...]
    weights = (m_old[:seqs] - lam * m_old[seqs:]).astype(BF16).astype(F32)
    w_new = (m_new[:seqs] - lam * m_new[seqs:]).astype(BF16).astype(F32)
    w_pair = iota((seqs, cache), 0) // 2
    copies[6].wait()

    def value_step(p, acc):
        lhs = jnp.where(w_pair == p, weights, 0.0).astype(BF16)
        rhs = jnp.concatenate([vals[2 * p], vals[2 * p + 1]], axis=1)
        return acc + jnp.dot(lhs, rhs, preferred_element_type=F32)

    mix = lax.fori_loop(0, seqs // 2, value_step, jnp.zeros((seqs, 2 * hd), F32))
    head_mix = jnp.where(iota((seqs, hd), 0) % 2 == 0, mix[:, :hd], mix[:, hd:])
    head_mix = head_mix + w_new * fresh_v.astype(F32)
    copies[7].wait()
    head_out = head_mix * lax.rsqrt(jnp.mean(head_mix * head_mix, axis=-1, keepdims=True) + EPS)
    head_out = (head_out * head_gain[...]).astype(BF16)

    copies[8].wait()
    for i in range(n):
        term = jnp.dot(head_out, wo[:, i * cols : (i + 1) * cols], preferred_element_type=F32)
        send_c[i] = term.astype(BF16)
    recv_c[tp] = send_c[tp]
    lax.fori_loop(1, n, c_start, 0)
    wait_all(c_arrived)
    attn_sum = jnp.sum(recv_c[...].astype(F32), axis=0)
    own_cols = pl.ds(pl.multiple_of(tp * cols, cols), cols)
    resid = tokens[:, own_cols].astype(F32) + attn_sum

    squares = jnp.broadcast_to(jnp.sum(resid * resid, axis=-1, keepdims=True), (seqs, 128))
    first = (tall_kind == 0) | (tall_kind == 2)
    second = (tall_kind == 1) | (tall_kind == 3)
    packed = exact_dot(jnp.where(first, dispatch, 0.0), resid[:, :128])
    packed += exact_dot(jnp.where(second, dispatch, 0.0), resid[:, 128:])
    packed += exact_dot(jnp.where(tall_kind >= 4, dispatch, 0.0), squares)
    send_e[...] = packed
    recv_e[pl.ds(pl.multiple_of(ep * 8, 8), 8), :] = send_e[pl.ds(pl.multiple_of(ep * 8, 8), 8), :]

    lax.fori_loop(1, n, e_start, 0)
    wait_all(e_arrived)

    def tile_row(ref, j):
        return ref[pl.ds(j, n, stride=8), :]

    token_rows = [
        jnp.concatenate([tile_row(recv_e, 2 * r), tile_row(recv_e, 2 * r + 1)], axis=1) for r in range(2)
    ]
    slab = jnp.concatenate(token_rows, axis=0)
    copies[9].wait()
    send_f[...] = (slab * moe_gain[:, own_cols]).astype(BF16)
    on_lane = iota((n, 128), 0) == iota((n, 128), 1)
    on_next = iota((n, 128), 0) + n == iota((n, 128), 1)
    stat = jnp.where(on_lane, tile_row(recv_e, 4), 0.0) + jnp.where(on_next, tile_row(recv_e, 5), 0.0)
    send_s[...] = jnp.broadcast_to(jnp.sum(stat, axis=0, keepdims=True), (8, 128))
    recv_f[tp] = send_f[...]
    recv_s[tp] = send_s[...]

    lax.fori_loop(1, n, s_start, 0)
    lax.fori_loop(1, n, f_start, 0)
    for i in (10, 11):
        copies[i].wait()
    slots = 2 * n

    def up_block(peer):
        at = pl.ds(pl.multiple_of(peer * cols, cols), cols)
        return jnp.dot(recv_f[peer], wgu[at, :], preferred_element_type=F32)

    def up_step(d, acc):
        f_arrived(d)
        return acc + up_block(lax.rem(tp + d, n))

    gate_up = lax.fori_loop(1, n, up_step, up_block(tp))
    wait_all(s_arrived)
    stats = jnp.sum(recv_s[...], axis=0)
    eye_slots = (iota((slots, 128), 0) == iota((slots, 128), 1)).astype(F32)
    sums = exact_dot(eye_slots, stats, NT)[:, 0:1]
    norm_scale = lax.rsqrt(sums / width + EPS)
    gate = gate_up[:, :hd] * norm_scale
    upper = gate_up[:, hd:] * norm_scale
    hidden = (gate / (1.0 + jnp.exp(-gate)) * upper).astype(BF16)

    copies[12].wait()
    for i in range(n):
        down = jnp.dot(hidden, wd[:, i * cols : (i + 1) * cols], preferred_element_type=F32)
        send_g[i] = down.astype(BF16)
    recv_g[tp] = send_g[tp]
    lax.fori_loop(1, n, g_start, 0)
    wait_all(g_arrived)
    expert_out = jnp.sum(recv_g[...].astype(F32), axis=0).astype(BF16).astype(F32)

    send_h[...] = jnp.zeros_like(send_h)
    for r in range(2):
        for h in range(2):
            send_h[pl.ds(2 * r + h, n, stride=8), :] = expert_out[r * n : (r + 1) * n, h * 128 : (h + 1) * 128]
    recv_h[pl.ds(pl.multiple_of(ep * 8, 8), 8), :] = send_h[pl.ds(pl.multiple_of(ep * 8, 8), 8), :]
    lax.fori_loop(1, n, h_start, 0)
    wait_all(h_arrived)
    back = recv_h[...]
    routed = [exact_dot(jnp.where(wide_kind % 2 == h, combine, 0.0), back) for h in range(2)]
    mixed_ref[...] = (resid + jnp.concatenate(routed, axis=1)).astype(BF16)

    for sent in (a_sent, b_sent, c_sent, e_sent, f_sent, s_sent, g_sent, h_sent):
        lax.fori_loop(1, n, sent, 0)


def on_device(n, *args):
    (tokens, attn_gain, w_query, w_key, w_value, mix_lambda, head_gain, w_output, cache_keys, cache_value) = args[:10]
    (lengths, moe_gain, group_ids, member_ids, group_gate, member_logits, w_exp_gate, w_exp_up, w_exp_down) = args[10:]
    seqs, width = tokens.shape
    cols = width // n
    hd = w_query.shape[1]
    cache = cache_keys.shape[1]
    operands = (
        tokens,
        attn_gain.reshape(1, width),
        w_query,
        w_key,
        w_value,
        mix_lambda.reshape(1, 1),
        head_gain.reshape(1, hd),
        w_output,
        cache_keys,
        cache_value,
        lengths.reshape(1, seqs),
        moe_gain.reshape(1, width),
        group_ids.reshape(1, seqs),
        member_ids.T,
        group_gate.reshape(1, seqs),
        member_logits.T,
        w_exp_gate,
        w_exp_up,
        w_exp_down,
    )
    small = (5, 10, 12, 13, 14, 15)
    vmem = pl.BlockSpec(memory_space=pltpu.VMEM)
    hbm = pl.BlockSpec(memory_space=pl.ANY)
    scratch = [
        pltpu.VMEM((seqs, width), BF16),
        pltpu.VMEM((1, width), F32),
        pltpu.VMEM((w_query.shape[0], 3 * hd), BF16),
        pltpu.VMEM((1, hd), F32),
        pltpu.VMEM((hd, width), BF16),
        pltpu.VMEM((seqs, cache, hd), BF16),
        pltpu.VMEM((seqs, cache, hd), BF16),
        pltpu.VMEM((1, width), F32),
        pltpu.VMEM((width, 2 * hd), BF16),
        pltpu.VMEM((hd, width), BF16),
        pltpu.VMEM((8, 128), F32),
        pltpu.VMEM((n, seqs, cols), BF16),
        pltpu.VMEM((n, seqs, cols), BF16),
        pltpu.VMEM((n, seqs, 3 * hd), F32),
        pltpu.VMEM((n, seqs, 3 * hd), F32),
        pltpu.VMEM((n, seqs, cols), BF16),
        pltpu.VMEM((n, seqs, cols), BF16),
        pltpu.VMEM((8 * n, 128), F32),
        pltpu.VMEM((8 * n, 128), F32),
        pltpu.VMEM((2 * n, cols), BF16),
        pltpu.VMEM((n, 2 * n, cols), BF16),
        pltpu.VMEM((8, 128), F32),
        pltpu.VMEM((n, 8, 128), F32),
        pltpu.VMEM((n, 2 * n, cols), BF16),
        pltpu.VMEM((n, 2 * n, cols), BF16),
        pltpu.VMEM((8 * n, 128), F32),
        pltpu.VMEM((8 * n, 128), F32),
        pltpu.SemaphoreType.DMA((13,)),
        pltpu.SemaphoreType.DMA((8, n)),
        pltpu.SemaphoreType.DMA((8, n)),
    ]
    return pl.pallas_call(
        functools.partial(layer_kernel, n),
        out_shape=(
            jax.ShapeDtypeStruct((seqs, cols), BF16),
            jax.ShapeDtypeStruct((seqs, hd), BF16),
            jax.ShapeDtypeStruct((seqs, hd), BF16),
        ),
        in_specs=[vmem if i in small else hbm for i in range(len(operands))],
        out_specs=(vmem, vmem, vmem),
        scratch_shapes=scratch,
        compiler_params=pltpu.CompilerParams(collective_id=0, has_side_effects=True),
        name="layer",
    )(*operands)


def solution(mesh):
    n = mesh.shape["ep"]
    return jax.shard_map(
        functools.partial(on_device, n),
        mesh=mesh,
        in_specs=(
            P("ep", None),
            P(),
            P("ep", "tp"),
            P("ep", "tp"),
            P("ep", "tp"),
            P("tp"),
            P(),
            P("tp", None),
            P("ep", None, "tp"),
            P("ep", None, "tp"),
            P("ep"),
            P(),
            P("ep"),
            P("ep", None),
            P("ep"),
            P("ep", None),
            P("ep", None, "tp"),
            P("ep", None, "tp"),
            P("ep", "tp", None),
        ),
        out_specs=(P("ep", "tp"), P("ep", "tp"), P("ep", "tp")),
        check_vma=False,
    )
```

```python
import functools

import jax
import jax.numpy as jnp
from jax import lax
from jax.experimental import pallas as pl
from jax.experimental.pallas import tpu as pltpu
from jax.sharding import PartitionSpec as P

EPG = 2
EPS = 1e-06
MESH = pl.DeviceIdType.MESH
HIGHEST = lax.Precision.HIGHEST
F32 = jnp.float32
BF16 = jnp.bfloat16
NT = (((1,), (1,)), ((), ()))


def iota(shape, dim):
    return lax.broadcasted_iota(jnp.int32, shape, dim)


def exact_dot(a, b, dims=(((1,), (0,)), ((), ()))):
    return lax.dot_general(a, b, dims, precision=HIGHEST, preferred_element_type=F32)


def layer_kernel(
    n,
    tokens_h,
    attn_gain_h,
    wq_h,
    wk_h,
    wv_h,
    lam_h,
    head_gain_h,
    wo_h,
    keys_h,
    vals_h,
    lengths_h,
    moe_gain_h,
    groups_h,
    members_h,
    gates_h,
    logits_h,
    wg_h,
    wu_h,
    wd_h,
    out_ref,
    tokens,
    attn_gain,
    wqkv,
    lam_ref,
    lengths_ref,
    groups_ref,
    members_ref,
    gates_ref,
    logits_ref,
    head_gain,
    wo,
    keys,
    vals,
    moe_gain,
    wgu,
    wd,
    rows_s,
    send_a,
    recv_a,
    send_b,
    recv_b,
    send_c,
    recv_c,
    send_e,
    recv_e,
    send_f,
    recv_f,
    send_s,
    recv_s,
    pair_out,
    pair_in,
    pair_own,
    send_g,
    recv_g,
    send_h,
    recv_h,
    load_sem,
    ss,
    rs,
):
    ep = lax.axis_index("ep")
    tp = lax.axis_index("tp")
    width = tokens_h.shape[1]
    cols = width // n
    seqs = tokens_h.shape[0]
    hd = wq_h.shape[1]
    half = hd // 2
    cache = keys_h.shape[1]

    barrier = pltpu.get_barrier_semaphore()

    def greet(d, carry):
        pl.semaphore_signal(barrier, inc=1, device_id=(lax.rem(ep + d, n), tp), device_id_type=MESH)
        pl.semaphore_signal(barrier, inc=1, device_id=(ep, lax.rem(tp + d, n)), device_id_type=MESH)
        return carry

    lax.fori_loop(1, n, greet, 0)

    loads = {
        "tokens": (tokens_h, tokens),
        "attn_gain": (attn_gain_h, attn_gain),
        "wq": (wq_h, wqkv.at[:, pl.ds(0, hd)]),
        "wk": (wk_h, wqkv.at[:, pl.ds(hd, hd)]),
        "wv": (wv_h, wqkv.at[:, pl.ds(2 * hd, hd)]),
        "lengths": (lengths_h, lengths_ref),
        "groups": (groups_h, groups_ref),
        "members": (members_h, members_ref),
        "gates": (gates_h, gates_ref),
        "logits": (logits_h, logits_ref),
        "head_gain": (head_gain_h, head_gain),
        "moe_gain": (moe_gain_h, moe_gain),
        "keys": (keys_h, keys),
        "vals": (vals_h, vals),
        "wo": (wo_h, wo),
        "wg": (wg_h.at[0], wgu.at[:, pl.ds(0, hd)]),
        "wu": (wu_h.at[0], wgu.at[:, pl.ds(hd, hd)]),
        "wd": (wd_h.at[0], wd),
    }
    copies = {
        name: pltpu.make_async_copy(source, target, load_sem.at[i])
        for i, (name, (source, target)) in enumerate(loads.items())
    }
    late = ("keys", "vals", "wo", "wg", "wu", "wd")
    for name, copy in copies.items():
        if name not in late:
            copy.start()

    def far_first(over_ep):
        if over_ep:
            side = 4
            offsets = [(a, b) for a in range(side) for b in range(n // side) if (a, b) != (0, 0)]
            offsets.sort(key=lambda o: -(min(o[0], side - o[0]) + min(o[1], n // side - o[1])))
            for a, b in offsets:
                yield lax.rem(ep // side + a, side) * side + lax.rem(ep % side + b, side)
        else:
            chips = n // 2
            offsets = [(a, b) for a in range(chips) for b in range(2) if (a, b) != (0, 0)]
            offsets.sort(key=lambda o: -min(o[0], chips - o[0]))
            for a, b in offsets:
                yield lax.rem(tp // 2 + a, chips) * 2 + lax.rem(tp % 2 + b, 2)

    def block(ref, i, tiles):
        return ref.at[pl.ds(pl.multiple_of(i * 8, 8), 8), :] if tiles else ref.at[i]

    def exchange(phase, send, recv, over_ep, whole=False, tiles=False):
        me = ep if over_ep else tp

        def descriptor(peer, incoming):
            slot = peer if incoming else me
            target = (peer, tp) if over_ep else (ep, peer)
            return pltpu.make_async_remote_copy(
                src_ref=send if whole else block(send, peer, tiles),
                dst_ref=block(recv, slot, tiles),
                send_sem=ss.at[phase, peer],
                recv_sem=rs.at[phase, slot],
                device_id=target,
                device_id_type=MESH,
            )

        def start():
            for peer in far_first(over_ep):
                descriptor(peer, False).start()

        def arrived(d):
            descriptor(lax.rem(me + d, n), True).wait_recv()

        def sent(d, carry):
            descriptor(lax.rem(me + d, n), False).wait_send()
            return carry

        return start, arrived, sent

    def wait_all(arrived):
        def body(d, carry):
            arrived(d)
            return carry

        lax.fori_loop(1, n, body, 0)

    a_start, a_arrived, a_sent = exchange(0, send_a, recv_a, True)
    b_start, b_arrived, b_sent = exchange(1, send_b, recv_b, True)
    c_start, c_arrived, c_sent = exchange(2, send_c, recv_c, False)
    e_start, e_arrived, e_sent = exchange(3, send_e, recv_e, True, tiles=True)
    s_start, s_arrived, s_sent = exchange(5, send_s, recv_s, False, True)
    h_start, h_arrived, h_sent = exchange(7, send_h, recv_h, True, tiles=True)

    copies["tokens"].wait()
    copies["attn_gain"].wait()
    x = tokens[...].astype(F32)
    normed = x * lax.rsqrt(jnp.mean(x * x, axis=-1, keepdims=True) + EPS) * attn_gain[...]
    normed = normed.astype(BF16)
    for i in range(n):
        send_a[i] = normed[:, i * cols : (i + 1) * cols]
    recv_a[ep] = send_a[ep]
    pl.semaphore_wait(barrier, 2 * (n - 1))
    a_start()
    for name in late:
        copies[name].start()

    for name in ("lengths", "groups", "members", "gates", "logits"):
        copies[name].wait()
    rows_s[...] = jnp.zeros_like(rows_s)
    rows_s[0:1, 0:seqs] = lengths_ref[...].astype(F32)
    rows_s[1:2, 0:seqs] = groups_ref[...].astype(F32)
    rows_s[2:4, 0:seqs] = members_ref[...].astype(F32)
    rows_s[4:5, 0:seqs] = gates_ref[...]
    rows_s[5:7, 0:seqs] = logits_ref[...]
    rows = rows_s[...][:, 0:seqs]
    eye = (iota((seqs, seqs), 0) == iota((seqs, seqs), 1)).astype(F32)
    columns = exact_dot(eye, rows, NT)
    id0_row = rows[1:2] * EPG + rows[2:3]
    id1_row = rows[1:2] * EPG + rows[3:4]
    id0_col = columns[:, 1:2] * EPG + columns[:, 2:3]
    id1_col = columns[:, 1:2] * EPG + columns[:, 3:4]
    logit_max = jnp.maximum(columns[:, 5:6], columns[:, 6:7])
    exp0 = jnp.exp(columns[:, 5:6] - logit_max)
    exp1 = jnp.exp(columns[:, 6:7] - logit_max)
    exp_sum = exp0 + exp1
    share0 = exp0 / exp_sum * columns[:, 4:5]
    share1 = exp1 / exp_sum * columns[:, 4:5]
    tall = 8 * n
    tall_row = iota((tall, seqs), 0)
    tall_expert = (tall_row // 8).astype(F32)
    tall_kind = tall_row % 8
    tall_rank = jnp.where((tall_kind == 2) | (tall_kind == 3) | (tall_kind == 5), 1.0, 0.0)
    chosen = ((id0_row == tall_expert) | (id1_row == tall_expert)).astype(F32)
    before = (iota((seqs, seqs), 0) < iota((seqs, seqs), 1)).astype(F32)
    rank = exact_dot(chosen, before)
    dispatch = jnp.where((rank == tall_rank) & (tall_kind < 6), chosen, 0.0)
    wide_col = iota((seqs, tall), 1)
    wide_expert = (wide_col // 8).astype(F32)
    wide_kind = wide_col % 8
    wide_rank = jnp.where(wide_kind >= 2, 1.0, 0.0)
    hit0 = (id0_col == wide_expert).astype(F32)
    hit1 = (id1_col == wide_expert).astype(F32)
    after = (iota((seqs, seqs), 1) < iota((seqs, seqs), 0)).astype(F32)
    wide_ranks = exact_dot(after, hit0 + hit1)
    combine = jnp.where((wide_ranks == wide_rank) & (wide_kind < 4), hit0 * share0 + hit1 * share1, 0.0)

    wait_all(a_arrived)
    for name in ("wq", "wk", "wv"):
        copies[name].wait()
    everyone = recv_a[...].reshape(n * seqs, cols)
    partial = jnp.dot(everyone, wqkv[...], preferred_element_type=F32)
    send_b[...] = partial.reshape(n, seqs, 3 * hd)
    recv_b[ep] = send_b[ep]
    b_start()
    wait_all(b_arrived)
    projected = jnp.sum(recv_b[...], axis=0).astype(BF16)
    query = projected[:, 0:hd]
    fresh_k = projected[:, hd : 2 * hd]
    fresh_v = projected[:, 2 * hd : 3 * hd]
    out_ref[:, cols:] = projected[:, hd:]

    total_heads = n
    slope = jnp.float32(0.0)
    for h in range(total_heads):
        slope = jnp.where(tp == h, jnp.float32(2.0 ** (-8.0 * (h + 1.0) / total_heads)), slope)
    scale = half ** (-0.5)
    both = 2 * seqs
    q2 = jnp.concatenate([query, query], axis=0).astype(F32)
    k2 = jnp.concatenate([fresh_k, fresh_k], axis=0).astype(F32)
    own_map = (iota((both, hd), 0) // seqs) == (iota((both, hd), 1) // half)
    q2 = jnp.where(own_map, q2, 0.0)
    new = jnp.sum(q2 * k2, axis=-1, keepdims=True) * scale
    q4 = jnp.concatenate([q2, q2], axis=1)
    q4_seq = iota((both, 2 * hd), 0) % seqs
    q4_side = iota((both, 2 * hd), 1) // hd
    copies["keys"].wait()

    def score_step(p, acc):
        lhs = jnp.where(q4_seq == 2 * p + q4_side, q4, 0.0).astype(BF16)
        rhs = jnp.concatenate([keys[2 * p], keys[2 * p + 1]], axis=1)
        return acc + lax.dot_general(lhs, rhs, NT, preferred_element_type=F32)

    old = jnp.zeros((both, cache), F32)
    for p in range(seqs // 2):
        old = score_step(p, old)
    old = old * scale
    count = jnp.concatenate([columns[:, 0:1], columns[:, 0:1]], axis=0)
    place = iota((both, cache), 1).astype(F32)
    old = jnp.where(place < count, old - slope * (count - place), -jnp.inf)
    top = jnp.maximum(jnp.max(old, axis=-1, keepdims=True), new)
    e_old = jnp.exp(old - top)
    e_new = jnp.exp(new - top)
    norm = jnp.sum(e_old, axis=-1, keepdims=True) + e_new
    m_old = e_old / norm
    m_new = e_new / norm
    lam = lam_h[0]
    weights = (m_old[:seqs] - lam * m_old[seqs:]).astype(BF16).astype(F32)
    w_new = (m_new[:seqs] - lam * m_new[seqs:]).astype(BF16).astype(F32)
    w_pair = iota((seqs, cache), 0) // 2
    copies["vals"].wait()

    def value_step(p, acc):
        lhs = jnp.where(w_pair == p, weights, 0.0).astype(BF16)
        rhs = jnp.concatenate([vals[2 * p], vals[2 * p + 1]], axis=1)
        return acc + jnp.dot(lhs, rhs, preferred_element_type=F32)

    mix = jnp.zeros((seqs, 2 * hd), F32)
    for p in range(seqs // 2):
        mix = value_step(p, mix)
    head_mix = jnp.where(iota((seqs, hd), 0) % 2 == 0, mix[:, :hd], mix[:, hd:])
    head_mix = head_mix + w_new * fresh_v.astype(F32)
    copies["head_gain"].wait()
    head_out = head_mix * lax.rsqrt(jnp.mean(head_mix * head_mix, axis=-1, keepdims=True) + EPS)
    head_out = (head_out * head_gain[...]).astype(BF16)

    copies["wo"].wait()
    for i in range(n):
        term = jnp.dot(head_out, wo[:, i * cols : (i + 1) * cols], preferred_element_type=F32)
        send_c[i] = term.astype(BF16)
    recv_c[tp] = send_c[tp]
    c_start()
    wait_all(c_arrived)
    attn_sum = jnp.sum(recv_c[...].astype(F32), axis=0)
    own_cols = pl.ds(pl.multiple_of(tp * cols, cols), cols)
    resid = tokens[:, own_cols].astype(F32) + attn_sum

    squares = jnp.broadcast_to(jnp.sum(resid * resid, axis=-1, keepdims=True), (seqs, 128))
    first = (tall_kind == 0) | (tall_kind == 2)
    second = (tall_kind == 1) | (tall_kind == 3)
    packed = exact_dot(jnp.where(first, dispatch, 0.0), resid[:, :128])
    packed += exact_dot(jnp.where(second, dispatch, 0.0), resid[:, 128:])
    packed += exact_dot(jnp.where(tall_kind >= 4, dispatch, 0.0), squares)
    send_e[...] = packed
    recv_e[pl.ds(pl.multiple_of(ep * 8, 8), 8), :] = send_e[pl.ds(pl.multiple_of(ep * 8, 8), 8), :]

    e_start()
    wait_all(e_arrived)

    def tile_row(ref, j):
        return ref[pl.ds(j, n, stride=8), :]

    token_rows = [
        jnp.concatenate([tile_row(recv_e, 2 * r), tile_row(recv_e, 2 * r + 1)], axis=1) for r in range(2)
    ]
    slab = jnp.concatenate(token_rows, axis=0)
    copies["moe_gain"].wait()
    send_f[...] = (slab * moe_gain[:, own_cols]).astype(BF16)
    on_lane = iota((n, 128), 0) == iota((n, 128), 1)
    on_next = iota((n, 128), 0) + n == iota((n, 128), 1)
    stat = jnp.where(on_lane, tile_row(recv_e, 4), 0.0) + jnp.where(on_next, tile_row(recv_e, 5), 0.0)
    send_s[...] = jnp.sum(stat, axis=0, keepdims=True)
    recv_f[tp] = send_f[...]
    recv_s[tp] = send_s[...]

    partner = tp + 1 - 2 * lax.rem(tp, 2)
    core = lax.rem(tp, 2)
    chips = n // 2
    chip = tp // 2
    z_order = sorted(range(1, chips), key=lambda a: -min(a, chips - a))

    def row_copy(source, slot, target, lane):
        return pltpu.make_async_remote_copy(
            src_ref=source,
            dst_ref=recv_f.at[slot],
            send_sem=ss.at[4, lane],
            recv_sem=rs.at[4, slot],
            device_id=(ep, target),
            device_id_type=MESH,
        )

    def z_peer(a):
        return lax.rem(chip + a, chips) * 2 + core

    outgoing = [row_copy(send_f, tp, z_peer(a), a) for a in z_order]
    outgoing.append(row_copy(send_f, tp, partner, 0))
    for copy in outgoing:
        copy.start()
    s_start()
    for a in reversed(z_order):
        slot = z_peer(a)
        row_copy(send_f, slot, slot, a).wait_recv()
        copy = row_copy(recv_f.at[slot], slot, partner, chips + a)
        copy.start()
        outgoing.append(copy)
    for name in ("wg", "wu"):
        copies[name].wait()
    slots = 2 * n
    for a in range(chips):
        slot = lax.rem(chip + a, chips) * 2 + 1 - core
        row_copy(send_f, slot, partner, a).wait_recv()
    everything = jnp.concatenate([recv_f[i] for i in range(n)], axis=1)
    gate_up = jnp.dot(everything, wgu[...], preferred_element_type=F32)
    wait_all(s_arrived)
    stats = jnp.broadcast_to(jnp.sum(recv_s[...], axis=0), (8, 128))
    eye_slots = (iota((slots, 128), 0) == iota((slots, 128), 1)).astype(F32)
    sums = exact_dot(eye_slots, stats, NT)[:, 0:1]
    norm_scale = lax.rsqrt(sums / width + EPS)
    gate = gate_up[:, :hd] * norm_scale
    upper = gate_up[:, hd:] * norm_scale
    hidden = (gate / (1.0 + jnp.exp(-gate)) * upper).astype(BF16)

    copies["wd"].wait()

    def down_block(z, c):
        at = pl.ds(pl.multiple_of((2 * z + c) * cols, cols), cols)
        return jnp.dot(hidden, wd[:, at], preferred_element_type=F32)

    for z in range(chips):
        pair_out[z] = down_block(z, 1 - core).astype(BF16)
    pair_copy = pltpu.make_async_remote_copy(
        src_ref=pair_out,
        dst_ref=pair_in,
        send_sem=ss.at[6, 0],
        recv_sem=rs.at[6, 0],
        device_id=(ep, partner),
        device_id_type=MESH,
    )
    pair_copy.start()
    outgoing.append(pair_copy)
    for z in range(chips):
        pair_own[z] = down_block(z, core)
    pair_copy.wait_recv()
    send_g[...] = (pair_own[...] + pair_in[...].astype(F32)).astype(BF16)
    recv_g[chip] = send_g[chip]

    def sum_copy(a, slot):
        return pltpu.make_async_remote_copy(
            src_ref=send_g.at[lax.rem(chip + a, chips)],
            dst_ref=recv_g.at[slot],
            send_sem=ss.at[6, a],
            recv_sem=rs.at[6, 1 + slot],
            device_id=(ep, z_peer(a)),
            device_id_type=MESH,
        )

    for a in z_order:
        copy = sum_copy(a, chip)
        copy.start()
        outgoing.append(copy)
    for a in reversed(z_order):
        sum_copy(a, lax.rem(chip + a, chips)).wait_recv()
    expert_out = jnp.sum(recv_g[...].astype(F32), axis=0).astype(BF16).astype(F32)

    send_h[...] = jnp.zeros_like(send_h)
    for r in range(2):
        for h in range(2):
            send_h[pl.ds(2 * r + h, n, stride=8), :] = expert_out[r * n : (r + 1) * n, h * 128 : (h + 1) * 128]
    recv_h[pl.ds(pl.multiple_of(ep * 8, 8), 8), :] = send_h[pl.ds(pl.multiple_of(ep * 8, 8), 8), :]
    h_start()
    wait_all(h_arrived)
    back = recv_h[...]
    routed = [exact_dot(jnp.where(wide_kind % 2 == h, combine, 0.0), back) for h in range(2)]
    out_ref[:, :cols] = (resid + jnp.concatenate(routed, axis=1)).astype(BF16)

    for sent in (a_sent, b_sent, c_sent, e_sent, s_sent, h_sent):
        lax.fori_loop(1, n, sent, 0)
    for copy in outgoing:
        copy.wait_send()


def unpack_kernel(packed_ref, mixed_ref, fresh_k_ref, fresh_v_ref, sems):
    copies = []
    at = 0
    for i, ref in enumerate((mixed_ref, fresh_k_ref, fresh_v_ref)):
        size = ref.shape[1]
        copies.append(pltpu.make_async_copy(packed_ref.at[:, pl.ds(at, size)], ref, sems.at[i]))
        at += size
    for copy in copies:
        copy.start()
    for copy in copies:
        copy.wait()


def on_device(n, *args):
    (tokens, attn_gain, w_query, w_key, w_value, mix_lambda, head_gain, w_output, cache_keys, cache_value) = args[:10]
    (lengths, moe_gain, group_ids, member_ids, group_gate, member_logits, w_exp_gate, w_exp_up, w_exp_down) = args[10:]
    seqs, width = tokens.shape
    cols = width // n
    hd = w_query.shape[1]
    cache = cache_keys.shape[1]
    operands = (
        tokens,
        attn_gain.reshape(1, width),
        w_query,
        w_key,
        w_value,
        mix_lambda,
        head_gain.reshape(1, hd),
        w_output,
        cache_keys,
        cache_value,
        lengths.reshape(1, seqs),
        moe_gain.reshape(1, width),
        group_ids.reshape(1, seqs),
        member_ids.T,
        group_gate.reshape(1, seqs),
        member_logits.T,
        w_exp_gate,
        w_exp_up,
        w_exp_down,
    )
    vmem = pl.BlockSpec(memory_space=pltpu.VMEM)
    hbm = pl.BlockSpec(memory_space=pl.ANY)
    scratch = [
        pltpu.VMEM((seqs, width), BF16),
        pltpu.VMEM((1, width), F32),
        pltpu.VMEM((w_query.shape[0], 3 * hd), BF16),
        pltpu.SMEM((1,), F32),
        pltpu.VMEM((1, seqs), jnp.int32),
        pltpu.VMEM((1, seqs), jnp.int32),
        pltpu.VMEM((2, seqs), jnp.int32),
        pltpu.VMEM((1, seqs), F32),
        pltpu.VMEM((2, seqs), F32),
        pltpu.VMEM((1, hd), F32),
        pltpu.VMEM((hd, width), BF16),
        pltpu.VMEM((seqs, cache, hd), BF16),
        pltpu.VMEM((seqs, cache, hd), BF16),
        pltpu.VMEM((1, width), F32),
        pltpu.VMEM((width, 2 * hd), BF16),
        pltpu.VMEM((hd, width), BF16),
        pltpu.VMEM((8, 128), F32),
        pltpu.VMEM((n, seqs, cols), BF16),
        pltpu.VMEM((n, seqs, cols), BF16),
        pltpu.VMEM((n, seqs, 3 * hd), F32),
        pltpu.VMEM((n, seqs, 3 * hd), F32),
        pltpu.VMEM((n, seqs, cols), BF16),
        pltpu.VMEM((n, seqs, cols), BF16),
        pltpu.VMEM((8 * n, 128), F32),
        pltpu.VMEM((8 * n, 128), F32),
        pltpu.VMEM((2 * n, cols), BF16),
        pltpu.VMEM((n, 2 * n, cols), BF16),
        pltpu.VMEM((1, 128), F32),
        pltpu.VMEM((n, 1, 128), F32),
        pltpu.VMEM((n // 2, 2 * n, cols), BF16),
        pltpu.VMEM((n // 2, 2 * n, cols), BF16),
        pltpu.VMEM((n // 2, 2 * n, cols), F32),
        pltpu.VMEM((n // 2, 2 * n, cols), BF16),
        pltpu.VMEM((n // 2, 2 * n, cols), BF16),
        pltpu.VMEM((8 * n, 128), F32),
        pltpu.VMEM((8 * n, 128), F32),
        pltpu.SemaphoreType.DMA((19,)),
        pltpu.SemaphoreType.DMA((8, n)),
        pltpu.SemaphoreType.DMA((8, n)),
    ]
    packed = pl.pallas_call(
        functools.partial(layer_kernel, n),
        out_shape=pltpu.VMEM((seqs, cols + 2 * hd), BF16),
        in_specs=[pl.BlockSpec(memory_space=pltpu.SMEM) if i == 5 else hbm for i in range(len(operands))],
        out_specs=vmem,
        scratch_shapes=scratch,
        compiler_params=pltpu.CompilerParams(collective_id=0, has_side_effects=True),
        name="layer",
    )(*operands)
    return pl.pallas_call(
        unpack_kernel,
        out_shape=(
            jax.ShapeDtypeStruct((seqs, cols), BF16),
            jax.ShapeDtypeStruct((seqs, hd), BF16),
            jax.ShapeDtypeStruct((seqs, hd), BF16),
        ),
        in_specs=[vmem],
        out_specs=(hbm, hbm, hbm),
        scratch_shapes=[pltpu.SemaphoreType.DMA((3,))],
        name="unpack",
    )(pltpu.with_memory_space_constraint(packed, pltpu.VMEM))


def solution(mesh):
    n = mesh.shape["ep"]
    return jax.shard_map(
        functools.partial(on_device, n),
        mesh=mesh,
        in_specs=(
            P("ep", None),
            P(),
            P("ep", "tp"),
            P("ep", "tp"),
            P("ep", "tp"),
            P("tp"),
            P(),
            P("tp", None),
            P("ep", None, "tp"),
            P("ep", None, "tp"),
            P("ep"),
            P(),
            P("ep"),
            P("ep", None),
            P("ep"),
            P("ep", None),
            P("ep", None, "tp"),
            P("ep", None, "tp"),
            P("ep", "tp", None),
        ),
        out_specs=(P("ep", "tp"), P("ep", "tp"), P("ep", "tp")),
        check_vma=False,
    )
```

```python
import functools

import jax
import jax.numpy as jnp
from jax import lax
from jax.experimental import pallas as pl
from jax.experimental.pallas import tpu as pltpu
from jax.sharding import PartitionSpec as P

EPG = 2
EPS = 1e-06
MESH = pl.DeviceIdType.MESH
HIGHEST = lax.Precision.HIGHEST
F32 = jnp.float32
BF16 = jnp.bfloat16
NT = (((1,), (1,)), ((), ()))


def iota(shape, dim):
    return lax.broadcasted_iota(jnp.int32, shape, dim)


def exact_dot(a, b, dims=(((1,), (0,)), ((), ()))):
    return lax.dot_general(a, b, dims, precision=HIGHEST, preferred_element_type=F32)


def layer_kernel(
    n,
    tokens_h,
    attn_gain_h,
    wq_h,
    wk_h,
    wv_h,
    lam_h,
    head_gain_h,
    wo_h,
    keys_h,
    vals_h,
    lengths_h,
    moe_gain_h,
    groups_h,
    members_h,
    gates_h,
    logits_h,
    wg_h,
    wu_h,
    wd_h,
    out_ref,
    tokens,
    attn_gain,
    wqkv,
    lam_ref,
    lengths_ref,
    groups_ref,
    members_ref,
    gates_ref,
    logits_ref,
    head_gain,
    wo,
    keys,
    vals,
    moe_gain,
    wgu,
    wd,
    rows_s,
    send_a,
    recv_a,
    send_b,
    recv_b,
    term_out,
    term_in,
    term_own,
    send_c,
    recv_c,
    send_e,
    recv_e,
    send_f,
    recv_f,
    send_s,
    stat_in,
    pair_s,
    recv_s,
    pair_out,
    pair_in,
    pair_own,
    send_g,
    recv_g,
    send_h,
    recv_h,
    load_sem,
    ss,
    rs,
):
    ep = lax.axis_index("ep")
    tp = lax.axis_index("tp")
    core = lax.rem(tp, 2)
    partner = tp + 1 - 2 * core
    chips = n // 2
    chip = tp // 2
    width = tokens_h.shape[1]
    cols = width // n
    seqs = tokens_h.shape[0]
    hd = wq_h.shape[1]
    half = hd // 2
    cache = keys_h.shape[1]

    side = 4
    ep_offsets = [(a, b) for a in range(side) for b in range(n // side) if (a, b) != (0, 0)]

    def ep_hops(o):
        return min(o[0], side - o[0]) + min(o[1], n // side - o[1])

    def ep_peer(o):
        return lax.rem(ep // side + o[0], side) * side + lax.rem(ep % side + o[1], side)

    ep_offsets.sort(key=lambda o: -ep_hops(o))
    ep_peers = [ep_peer(o) for o in ep_offsets]
    z_order = sorted(range(1, chips), key=lambda a: -min(a, chips - a))

    def z_peer(a):
        return lax.rem(chip + a, chips) * 2 + core

    loads = {
        "tokens": (tokens_h, tokens),
        "attn_gain": (attn_gain_h, attn_gain),
        "wq": (wq_h, wqkv.at[:, pl.ds(0, hd)]),
        "wk": (wk_h, wqkv.at[:, pl.ds(hd, hd)]),
        "wv": (wv_h, wqkv.at[:, pl.ds(2 * hd, hd)]),
        "lengths": (lengths_h, lengths_ref),
        "groups": (groups_h, groups_ref),
        "members": (members_h, members_ref),
        "gates": (gates_h, gates_ref),
        "logits": (logits_h, logits_ref),
        "head_gain": (head_gain_h, head_gain),
        "moe_gain": (moe_gain_h, moe_gain),
        "keys": (keys_h, keys),
        "vals": (vals_h, vals),
        "wo": (wo_h, wo),
        "wg": (wg_h.at[0], wgu.at[:, pl.ds(0, hd)]),
        "wu": (wu_h.at[0], wgu.at[:, pl.ds(hd, hd)]),
        "wd": (wd_h.at[0], wd),
    }
    copies = {
        name: pltpu.make_async_copy(source, target, load_sem.at[i])
        for i, (name, (source, target)) in enumerate(loads.items())
    }
    copies["tokens"].start()
    copies["attn_gain"].start()

    barrier = pltpu.get_barrier_semaphore()
    for peer in ep_peers:
        pl.semaphore_signal(barrier, inc=1, device_id=(peer, tp), device_id_type=MESH)
    for a in z_order:
        pl.semaphore_signal(barrier, inc=1, device_id=(ep, z_peer(a)), device_id_type=MESH)
    pl.semaphore_signal(barrier, inc=1, device_id=(ep, partner), device_id_type=MESH)

    late = ("keys", "vals", "wo", "wg", "wu", "wd")
    for name, copy in copies.items():
        if name not in late + ("tokens", "attn_gain"):
            copy.start()

    def exchange(phase, send, recv, tile_rows=None):
        def block(ref, i):
            return ref.at[i] if tile_rows is None else ref.at[pl.ds(pl.multiple_of(i * 8, 8), tile_rows), :]

        def descriptor(peer, incoming):
            return pltpu.make_async_remote_copy(
                src_ref=block(send, peer),
                dst_ref=block(recv, peer if incoming else ep),
                send_sem=ss.at[phase, peer],
                recv_sem=rs.at[phase, peer if incoming else ep],
                device_id=(peer, tp),
                device_id_type=MESH,
            )

        def start(peers):
            for peer in peers:
                descriptor(peer, False).start()

        def arrived(peer):
            descriptor(peer, True).wait_recv()

        def sent(d, carry):
            descriptor(lax.rem(ep + d, n), False).wait_send()
            return carry

        return start, arrived, sent

    def wait_all(arrived):
        def body(d, carry):
            arrived(lax.rem(ep + d, n))
            return carry

        lax.fori_loop(1, n, body, 0)

    outgoing = []

    def to_partner(phase, source, target):
        copy = pltpu.make_async_remote_copy(
            src_ref=source,
            dst_ref=target,
            send_sem=ss.at[phase, 0],
            recv_sem=rs.at[phase, n - 1],
            device_id=(ep, partner),
            device_id_type=MESH,
        )
        copy.start()
        outgoing.append(copy)
        return copy

    def along_z(phase, source, recv):
        def descriptor(a, slot):
            return pltpu.make_async_remote_copy(
                src_ref=source(lax.rem(chip + a, chips)),
                dst_ref=recv.at[slot],
                send_sem=ss.at[phase, a],
                recv_sem=rs.at[phase, slot],
                device_id=(ep, z_peer(a)),
                device_id_type=MESH,
            )

        for a in z_order:
            copy = descriptor(a, chip)
            copy.start()
            outgoing.append(copy)

        def wait():
            for a in reversed(z_order):
                descriptor(a, lax.rem(chip + a, chips)).wait_recv()

        return wait

    a_start, a_arrived, a_sent = exchange(0, send_a, recv_a)
    b_start, b_arrived, b_sent = exchange(1, send_b, recv_b)
    e_start, e_arrived, e_sent = exchange(3, send_e, recv_e, 6)
    h_start, h_arrived, h_sent = exchange(7, send_h, recv_h, 4)
    recv_h[...] = jnp.zeros_like(recv_h)

    copies["tokens"].wait()
    copies["attn_gain"].wait()
    x = tokens[...].astype(F32)
    normed = x * lax.rsqrt(jnp.mean(x * x, axis=-1, keepdims=True) + EPS) * attn_gain[...]
    normed = normed.astype(BF16)
    for i in range(n):
        send_a[i] = normed[:, i * cols : (i + 1) * cols]
    recv_a[ep] = send_a[ep]
    pl.semaphore_wait(barrier, n - 1 + chips)
    a_start(ep_peers)
    for name in late:
        copies[name].start()

    for name in ("lengths", "groups", "members", "gates", "logits"):
        copies[name].wait()
    rows_s[...] = jnp.zeros_like(rows_s)
    rows_s[0:1, 0:seqs] = lengths_ref[...].astype(F32)
    rows_s[1:2, 0:seqs] = groups_ref[...].astype(F32)
    rows_s[2:4, 0:seqs] = members_ref[...].astype(F32)
    rows_s[4:5, 0:seqs] = gates_ref[...]
    rows_s[5:7, 0:seqs] = logits_ref[...]
    rows = rows_s[...][:, 0:seqs]
    eye = (iota((seqs, seqs), 0) == iota((seqs, seqs), 1)).astype(F32)
    columns = exact_dot(eye, rows, NT)
    id0_row = rows[1:2] * EPG + rows[2:3]
    id1_row = rows[1:2] * EPG + rows[3:4]
    id0_col = columns[:, 1:2] * EPG + columns[:, 2:3]
    id1_col = columns[:, 1:2] * EPG + columns[:, 3:4]
    logit_max = jnp.maximum(columns[:, 5:6], columns[:, 6:7])
    exp0 = jnp.exp(columns[:, 5:6] - logit_max)
    exp1 = jnp.exp(columns[:, 6:7] - logit_max)
    exp_sum = exp0 + exp1
    share0 = exp0 / exp_sum * columns[:, 4:5]
    share1 = exp1 / exp_sum * columns[:, 4:5]
    tall = 8 * n
    tall_row = iota((tall, seqs), 0)
    tall_expert = (tall_row // 8).astype(F32)
    tall_kind = tall_row % 8
    tall_rank = jnp.where((tall_kind == 2) | (tall_kind == 3) | (tall_kind == 5), 1.0, 0.0)
    chosen = ((id0_row == tall_expert) | (id1_row == tall_expert)).astype(F32)
    before = (iota((seqs, seqs), 0) < iota((seqs, seqs), 1)).astype(F32)
    rank = exact_dot(chosen, before)
    dispatch = jnp.where((rank == tall_rank) & (tall_kind < 6), chosen, 0.0)
    first = (tall_kind == 0) | (tall_kind == 2)
    second = (tall_kind == 1) | (tall_kind == 3)
    kinds = [jnp.where(kind, dispatch, 0.0) for kind in (first, second, tall_kind >= 4)]
    routes = jnp.concatenate(kinds * 3, axis=1).astype(BF16)
    wide_col = iota((seqs, tall), 1)
    wide_expert = (wide_col // 8).astype(F32)
    wide_kind = wide_col % 8
    wide_rank = jnp.where(wide_kind >= 2, 1.0, 0.0)
    hit0 = (id0_col == wide_expert).astype(F32)
    hit1 = (id1_col == wide_expert).astype(F32)
    after = (iota((seqs, seqs), 1) < iota((seqs, seqs), 0)).astype(F32)
    wide_ranks = exact_dot(after, hit0 + hit1)
    combine = jnp.where((wide_ranks == wide_rank) & (wide_kind < 4), hit0 * share0 + hit1 * share1, 0.0)

    parts = []
    for h in range(2):
        rest = jnp.where(wide_kind % 2 == h, combine, 0.0)
        for _ in range(3):
            part = rest.astype(BF16)
            parts.append(part)
            rest = rest - part.astype(F32)
    shares = jnp.concatenate(parts, axis=0)

    for name in ("wq", "wk", "wv"):
        copies[name].wait()
    wait_all(a_arrived)
    everyone = recv_a[...].reshape(n * seqs, cols)
    partial = jnp.dot(everyone, wqkv[...], preferred_element_type=F32)
    send_b[...] = partial.reshape(n, seqs, 3 * hd)
    b_start(ep_peers)
    recv_b[ep] = send_b[ep]
    wait_all(b_arrived)
    projected = jnp.sum(recv_b[...], axis=0).astype(BF16)
    query = projected[:, 0:hd]
    fresh_k = projected[:, hd : 2 * hd]
    fresh_v = projected[:, 2 * hd : 3 * hd]
    out_ref[:, cols:] = projected[:, hd:]

    total_heads = n
    slope = jnp.float32(0.0)
    for h in range(total_heads):
        slope = jnp.where(tp == h, jnp.float32(2.0 ** (-8.0 * (h + 1.0) / total_heads)), slope)
    scale = half ** (-0.5)
    some = seqs // 2
    both = 2 * some
    q_all = query.astype(F32)
    k_all = fresh_k.astype(F32)
    v_all = fresh_v.astype(F32)
    own_map = (iota((both, hd), 0) // some) == (iota((both, hd), 1) // half)
    q4_seq = iota((both, 2 * hd), 0) % some
    q4_side = iota((both, 2 * hd), 1) // hd
    place = iota((both, cache), 1).astype(F32)
    mix_seq = iota((some, hd), 0)
    copies["keys"].wait()
    scores = []
    for part in range(2):
        at = slice(part * some, (part + 1) * some)
        q2 = jnp.where(own_map, jnp.concatenate([q_all[at], q_all[at]], axis=0), 0.0)
        q4 = jnp.concatenate([q2, q2], axis=1)
        old = jnp.zeros((both, cache), F32)
        for p in range(some // 2):
            lhs = jnp.where(q4_seq == 2 * p + q4_side, q4, 0.0).astype(BF16)
            b0 = part * some + 2 * p
            rhs = jnp.concatenate([keys[b0], keys[b0 + 1]], axis=1)
            old = old + lax.dot_general(lhs, rhs, NT, preferred_element_type=F32)
        scores.append((q2, old * scale))
    copies["vals"].wait()
    lam = lam_h[0]
    mixes = []
    for part, (q2, old) in enumerate(scores):
        at = slice(part * some, (part + 1) * some)
        new = jnp.sum(q2 * jnp.concatenate([k_all[at], k_all[at]], axis=0), axis=-1, keepdims=True) * scale
        count = jnp.concatenate([columns[at, 0:1], columns[at, 0:1]], axis=0)
        old = jnp.where(place < count, old - slope * (count - place), -jnp.inf)
        top = jnp.maximum(jnp.max(old, axis=-1, keepdims=True), new)
        e_old = jnp.exp(old - top)
        e_new = jnp.exp(new - top)
        norm = jnp.sum(e_old, axis=-1, keepdims=True) + e_new
        m_old = e_old / norm
        m_new = e_new / norm
        weights = (m_old[:some] - lam * m_old[some:]).astype(BF16)
        w_new = (m_new[:some] - lam * m_new[some:]).astype(BF16).astype(F32)
        mix = w_new * v_all[at]
        for p in range(some // 2):
            b0 = part * some + 2 * p
            pair = jnp.concatenate([vals[b0], vals[b0 + 1]], axis=1)
            both_mix = jnp.dot(weights, pair, preferred_element_type=F32)
            mix = mix + jnp.where(mix_seq == 2 * p, both_mix[:, :hd], 0.0)
            mix = mix + jnp.where(mix_seq == 2 * p + 1, both_mix[:, hd:], 0.0)
        mixes.append(mix)
    head_mix = jnp.concatenate(mixes, axis=0)
    copies["head_gain"].wait()
    head_out = head_mix * lax.rsqrt(jnp.mean(head_mix * head_mix, axis=-1, keepdims=True) + EPS)
    head_out = (head_out * head_gain[...]).astype(BF16)

    copies["wo"].wait()

    def term_block(z, c):
        at = pl.ds(pl.multiple_of((2 * z + c) * cols, cols), cols)
        return jnp.dot(head_out, wo[:, at], preferred_element_type=F32).astype(BF16)

    for z in range(chips):
        term_out[z] = term_block(z, 1 - core)
    term_copy = to_partner(2, term_out, term_in)
    for z in range(chips):
        term_own[z] = term_block(z, core).astype(F32)
    term_copy.wait_recv()
    send_c[...] = (term_own[...] + term_in[...].astype(F32)).astype(BF16)
    c_wait = along_z(2, lambda i: send_c.at[i], recv_c)
    recv_c[chip] = send_c[chip]
    c_wait()
    attn_sum = jnp.sum(recv_c[...].astype(F32), axis=0)
    own_cols = pl.ds(pl.multiple_of(tp * cols, cols), cols)
    resid = tokens[:, own_cols].astype(F32) + attn_sum

    squares = jnp.broadcast_to(jnp.sum(resid * resid, axis=-1, keepdims=True), (seqs, 128))
    rest = [resid[:, :128], resid[:, 128:], squares]
    parts = []
    for _ in range(3):
        part = [r.astype(BF16) for r in rest]
        rest = [r - p.astype(F32) for r, p in zip(rest, part)]
        parts += part
    packed = jnp.dot(routes, jnp.concatenate(parts, axis=0), preferred_element_type=F32)
    send_e[...] = packed
    recv_e[pl.ds(pl.multiple_of(ep * 8, 8), 8), :] = send_e[pl.ds(pl.multiple_of(ep * 8, 8), 8), :]

    e_start(ep_peers)
    wait_all(e_arrived)

    def tile_row(ref, j):
        return ref[pl.ds(j, n, stride=8), :]

    token_rows = [
        jnp.concatenate([tile_row(recv_e, 2 * r), tile_row(recv_e, 2 * r + 1)], axis=1) for r in range(2)
    ]
    slab = jnp.concatenate(token_rows, axis=0)
    copies["moe_gain"].wait()
    send_f[...] = (slab * moe_gain[:, own_cols]).astype(BF16)
    on_lane = iota((n, 128), 0) == iota((n, 128), 1)
    on_next = iota((n, 128), 0) + n == iota((n, 128), 1)
    stat = jnp.where(on_lane, tile_row(recv_e, 4), 0.0) + jnp.where(on_next, tile_row(recv_e, 5), 0.0)
    send_s[...] = jnp.sum(stat, axis=0, keepdims=True)
    recv_f[tp] = send_f[...]

    recv_s[chip] = send_s[...]
    s_wait = along_z(5, lambda i: send_s, recv_s)

    def row_copy(source, slot, target, lane):
        return pltpu.make_async_remote_copy(
            src_ref=source,
            dst_ref=recv_f.at[slot],
            send_sem=ss.at[4, lane],
            recv_sem=rs.at[4, slot],
            device_id=(ep, target),
            device_id_type=MESH,
        )

    rows_out = [row_copy(send_f, tp, z_peer(a), a) for a in z_order]
    rows_out.append(row_copy(send_f, tp, partner, 0))
    for copy in rows_out:
        copy.start()
    for a in reversed(z_order):
        slot = z_peer(a)
        row_copy(send_f, slot, slot, a).wait_recv()
        copy = row_copy(recv_f.at[slot], slot, partner, chips + a)
        copy.start()
        rows_out.append(copy)
    outgoing.extend(rows_out)
    for name in ("wg", "wu"):
        copies[name].wait()
    slots = 2 * n
    s_wait()
    pair_s[...] = jnp.sum(recv_s[...], axis=0)
    stat_copy = to_partner(5, pair_s, stat_in)
    for a in range(chips):
        slot = lax.rem(chip + a, chips) * 2 + 1 - core
        row_copy(send_f, slot, partner, a).wait_recv()
    everything = jnp.concatenate([recv_f[i] for i in range(n)], axis=1)
    gate_up = jnp.dot(everything, wgu[...], preferred_element_type=F32)
    stat_copy.wait_recv()
    stats = jnp.broadcast_to(pair_s[...] + stat_in[...], (8, 128))
    eye_slots = (iota((slots, 128), 0) == iota((slots, 128), 1)).astype(F32)
    sums = exact_dot(eye_slots, stats, NT)[:, 0:1]
    norm_scale = lax.rsqrt(sums / width + EPS)
    gate = gate_up[:, :hd] * norm_scale
    upper = gate_up[:, hd:] * norm_scale
    hidden = (gate / (1.0 + jnp.exp(-gate)) * upper).astype(BF16)

    copies["wd"].wait()

    def down_block(z, c):
        at = pl.ds(pl.multiple_of((2 * z + c) * cols, cols), cols)
        return jnp.dot(hidden, wd[:, at], preferred_element_type=F32)

    for z in range(chips):
        pair_out[z] = down_block(z, 1 - core).astype(BF16)
    pair_copy = to_partner(6, pair_out, pair_in)
    for z in range(chips):
        pair_own[z] = down_block(z, core)
    pair_copy.wait_recv()
    send_g[...] = (pair_own[...] + pair_in[...].astype(F32)).astype(BF16)
    g_wait = along_z(6, lambda i: send_g.at[i], recv_g)
    recv_g[chip] = send_g[chip]
    g_wait()
    expert_out = jnp.sum(recv_g[...].astype(F32), axis=0).astype(BF16).astype(F32)

    for r in range(2):
        for h in range(2):
            send_h[pl.ds(2 * r + h, n, stride=8), :] = expert_out[r * n : (r + 1) * n, h * 128 : (h + 1) * 128]
    recv_h[pl.ds(pl.multiple_of(ep * 8, 8), 4), :] = send_h[pl.ds(pl.multiple_of(ep * 8, 8), 4), :]
    h_start(ep_peers)
    wait_all(h_arrived)
    back = jnp.dot(shares, recv_h[...].astype(BF16), preferred_element_type=F32)
    routed = [sum(back[(3 * h + i) * seqs : (3 * h + i + 1) * seqs] for i in range(3)) for h in range(2)]
    out_ref[:, :cols] = (resid + jnp.concatenate(routed, axis=1)).astype(BF16)

    for sent in (a_sent, b_sent, e_sent, h_sent):
        lax.fori_loop(1, n, sent, 0)
    for copy in outgoing:
        copy.wait_send()


def unpack_kernel(packed_ref, mixed_ref, fresh_k_ref, fresh_v_ref, sems):
    copies = []
    at = 0
    for i, ref in enumerate((mixed_ref, fresh_k_ref, fresh_v_ref)):
        size = ref.shape[1]
        copies.append(pltpu.make_async_copy(packed_ref.at[:, pl.ds(at, size)], ref, sems.at[i]))
        at += size
    for copy in copies:
        copy.start()
    for copy in copies:
        copy.wait()


def on_device(n, *args):
    (tokens, attn_gain, w_query, w_key, w_value, mix_lambda, head_gain, w_output, cache_keys, cache_value) = args[:10]
    (lengths, moe_gain, group_ids, member_ids, group_gate, member_logits, w_exp_gate, w_exp_up, w_exp_down) = args[10:]
    seqs, width = tokens.shape
    cols = width // n
    hd = w_query.shape[1]
    cache = cache_keys.shape[1]
    operands = (
        tokens,
        attn_gain.reshape(1, width),
        w_query,
        w_key,
        w_value,
        mix_lambda,
        head_gain.reshape(1, hd),
        w_output,
        cache_keys,
        cache_value,
        lengths.reshape(1, seqs),
        moe_gain.reshape(1, width),
        group_ids.reshape(1, seqs),
        member_ids.T,
        group_gate.reshape(1, seqs),
        member_logits.T,
        w_exp_gate,
        w_exp_up,
        w_exp_down,
    )
    vmem = pl.BlockSpec(memory_space=pltpu.VMEM)
    hbm = pl.BlockSpec(memory_space=pl.ANY)
    scratch = [
        pltpu.VMEM((seqs, width), BF16),
        pltpu.VMEM((1, width), F32),
        pltpu.VMEM((w_query.shape[0], 3 * hd), BF16),
        pltpu.SMEM((1,), F32),
        pltpu.VMEM((1, seqs), jnp.int32),
        pltpu.VMEM((1, seqs), jnp.int32),
        pltpu.VMEM((2, seqs), jnp.int32),
        pltpu.VMEM((1, seqs), F32),
        pltpu.VMEM((2, seqs), F32),
        pltpu.VMEM((1, hd), F32),
        pltpu.VMEM((hd, width), BF16),
        pltpu.VMEM((seqs, cache, hd), BF16),
        pltpu.VMEM((seqs, cache, hd), BF16),
        pltpu.VMEM((1, width), F32),
        pltpu.VMEM((width, 2 * hd), BF16),
        pltpu.VMEM((hd, width), BF16),
        pltpu.VMEM((8, 128), F32),
        pltpu.VMEM((n, seqs, cols), BF16),
        pltpu.VMEM((n, seqs, cols), BF16),
        pltpu.VMEM((n, seqs, 3 * hd), F32),
        pltpu.VMEM((n, seqs, 3 * hd), F32),
        pltpu.VMEM((n // 2, seqs, cols), BF16),
        pltpu.VMEM((n // 2, seqs, cols), BF16),
        pltpu.VMEM((n // 2, seqs, cols), F32),
        pltpu.VMEM((n // 2, seqs, cols), BF16),
        pltpu.VMEM((n // 2, seqs, cols), BF16),
        pltpu.VMEM((8 * n, 128), F32),
        pltpu.VMEM((8 * n, 128), F32),
        pltpu.VMEM((2 * n, cols), BF16),
        pltpu.VMEM((n, 2 * n, cols), BF16),
        pltpu.VMEM((1, 128), F32),
        pltpu.VMEM((1, 128), F32),
        pltpu.VMEM((1, 128), F32),
        pltpu.VMEM((n // 2, 1, 128), F32),
        pltpu.VMEM((n // 2, 2 * n, cols), BF16),
        pltpu.VMEM((n // 2, 2 * n, cols), BF16),
        pltpu.VMEM((n // 2, 2 * n, cols), F32),
        pltpu.VMEM((n // 2, 2 * n, cols), BF16),
        pltpu.VMEM((n // 2, 2 * n, cols), BF16),
        pltpu.VMEM((8 * n, 128), F32),
        pltpu.VMEM((8 * n, 128), F32),
        pltpu.SemaphoreType.DMA((19,)),
        pltpu.SemaphoreType.DMA((8, n)),
        pltpu.SemaphoreType.DMA((8, n)),
    ]
    packed = pl.pallas_call(
        functools.partial(layer_kernel, n),
        out_shape=pltpu.VMEM((seqs, cols + 2 * hd), BF16),
        in_specs=[pl.BlockSpec(memory_space=pltpu.SMEM) if i == 5 else hbm for i in range(len(operands))],
        out_specs=vmem,
        scratch_shapes=scratch,
        compiler_params=pltpu.CompilerParams(collective_id=0, has_side_effects=True),
        name="layer",
    )(*operands)
    return pl.pallas_call(
        unpack_kernel,
        out_shape=(
            jax.ShapeDtypeStruct((seqs, cols), BF16),
            jax.ShapeDtypeStruct((seqs, hd), BF16),
            jax.ShapeDtypeStruct((seqs, hd), BF16),
        ),
        in_specs=[vmem],
        out_specs=(hbm, hbm, hbm),
        scratch_shapes=[pltpu.SemaphoreType.DMA((3,))],
        name="unpack",
    )(pltpu.with_memory_space_constraint(packed, pltpu.VMEM))


def solution(mesh):
    n = mesh.shape["ep"]
    return jax.shard_map(
        functools.partial(on_device, n),
        mesh=mesh,
        in_specs=(
            P("ep", None),
            P(),
            P("ep", "tp"),
            P("ep", "tp"),
            P("ep", "tp"),
            P("tp"),
            P(),
            P("tp", None),
            P("ep", None, "tp"),
            P("ep", None, "tp"),
            P("ep"),
            P(),
            P("ep"),
            P("ep", None),
            P("ep"),
            P("ep", None),
            P("ep", None, "tp"),
            P("ep", None, "tp"),
            P("ep", "tp", None),
        ),
        out_specs=(P("ep", "tp"), P("ep", "tp"), P("ep", "tp")),
        check_vma=False,
    )
```

```python
import functools

import jax
import jax.numpy as jnp
from jax import lax
from jax.experimental import pallas as pl
from jax.experimental.pallas import tpu as pltpu
from jax.sharding import PartitionSpec as P

EPG = 2
EPS = 1e-06
MESH = pl.DeviceIdType.MESH
HIGHEST = lax.Precision.HIGHEST
F32 = jnp.float32
BF16 = jnp.bfloat16
NT = (((1,), (1,)), ((), ()))


def iota(shape, dim):
    return lax.broadcasted_iota(jnp.int32, shape, dim)


def exact_dot(a, b, dims=(((1,), (0,)), ((), ()))):
    return lax.dot_general(a, b, dims, precision=HIGHEST, preferred_element_type=F32)


def layer_kernel(
    n,
    tokens_h,
    attn_gain_h,
    wq_h,
    wk_h,
    wv_h,
    lam_h,
    head_gain_h,
    wo_h,
    keys_h,
    vals_h,
    lengths_h,
    moe_gain_h,
    groups_h,
    members_h,
    gates_h,
    logits_h,
    wg_h,
    wu_h,
    wd_h,
    out_ref,
    tokens,
    attn_gain,
    wqkv,
    lam_ref,
    lengths_ref,
    groups_ref,
    members_ref,
    gates_ref,
    logits_ref,
    head_gain,
    wo,
    keys,
    vals,
    moe_gain,
    wgu,
    wd,
    rows_s,
    send_a,
    recv_a,
    send_b,
    recv_b,
    term_out,
    term_in,
    term_own,
    send_c,
    recv_c,
    send_e,
    recv_e,
    send_f,
    recv_f,
    send_s,
    stat_in,
    pair_s,
    recv_s,
    pair_out,
    pair_in,
    pair_own,
    send_g,
    recv_g,
    send_h,
    recv_h,
    load_sem,
    ss,
    rs,
):
    ep = lax.axis_index("ep")
    tp = lax.axis_index("tp")
    core = lax.rem(tp, 2)
    partner = tp + 1 - 2 * core
    chips = n // 2
    chip = tp // 2
    width = tokens_h.shape[1]
    cols = width // n
    seqs = tokens_h.shape[0]
    hd = wq_h.shape[1]
    half = hd // 2
    cache = keys_h.shape[1]

    side = 4
    ep_offsets = [(a, b) for a in range(side) for b in range(n // side) if (a, b) != (0, 0)]

    def ep_hops(o):
        return min(o[0], side - o[0]) + min(o[1], n // side - o[1])

    def ep_peer(o):
        return lax.rem(ep // side + o[0], side) * side + lax.rem(ep % side + o[1], side)

    ep_offsets.sort(key=lambda o: -ep_hops(o))
    ep_peers = [ep_peer(o) for o in ep_offsets]
    z_order = sorted(range(1, chips), key=lambda a: -min(a, chips - a))

    def z_peer(a):
        return lax.rem(chip + a, chips) * 2 + core

    loads = {
        "tokens": (tokens_h, tokens),
        "attn_gain": (attn_gain_h, attn_gain),
        "wq": (wq_h, wqkv.at[:, pl.ds(0, hd)]),
        "wk": (wk_h, wqkv.at[:, pl.ds(hd, hd)]),
        "wv": (wv_h, wqkv.at[:, pl.ds(2 * hd, hd)]),
        "lengths": (lengths_h, lengths_ref),
        "groups": (groups_h, groups_ref),
        "members": (members_h, members_ref),
        "gates": (gates_h, gates_ref),
        "logits": (logits_h, logits_ref),
        "head_gain": (head_gain_h, head_gain),
        "moe_gain": (moe_gain_h, moe_gain),
        "keys": (keys_h, keys),
        "vals": (vals_h, vals),
        "wo": (wo_h, wo),
        "wg": (wg_h.at[0], wgu.at[:, pl.ds(0, hd)]),
        "wu": (wu_h.at[0], wgu.at[:, pl.ds(hd, hd)]),
        "wd": (wd_h.at[0], wd),
    }
    copies = {
        name: pltpu.make_async_copy(source, target, load_sem.at[i])
        for i, (name, (source, target)) in enumerate(loads.items())
    }
    copies["tokens"].start()
    copies["attn_gain"].start()

    barrier = pltpu.get_barrier_semaphore()
    for peer in ep_peers:
        pl.semaphore_signal(barrier, inc=1, device_id=(peer, tp), device_id_type=MESH)
    for a in z_order:
        pl.semaphore_signal(barrier, inc=1, device_id=(ep, z_peer(a)), device_id_type=MESH)
    pl.semaphore_signal(barrier, inc=1, device_id=(ep, partner), device_id_type=MESH)

    late = ("keys", "vals", "wo", "wg", "wu", "wd")
    for name, copy in copies.items():
        if name not in late + ("tokens", "attn_gain"):
            copy.start()

    def exchange(phase, send, recv, tile_rows=None):
        def block(ref, i):
            return ref.at[i] if tile_rows is None else ref.at[pl.ds(pl.multiple_of(i * 8, 8), tile_rows), :]

        def descriptor(peer, incoming):
            return pltpu.make_async_remote_copy(
                src_ref=block(send, peer),
                dst_ref=block(recv, peer if incoming else ep),
                send_sem=ss.at[phase, peer],
                recv_sem=rs.at[phase, peer if incoming else ep],
                device_id=(peer, tp),
                device_id_type=MESH,
            )

        def start(peers):
            for peer in peers:
                descriptor(peer, False).start()

        def arrived(peer):
            descriptor(peer, True).wait_recv()

        def sent(d, carry):
            descriptor(lax.rem(ep + d, n), False).wait_send()
            return carry

        return start, arrived, sent

    def wait_all(arrived):
        def body(d, carry):
            arrived(lax.rem(ep + d, n))
            return carry

        lax.fori_loop(1, n, body, 0)

    outgoing = []

    def to_partner(phase, source, target):
        copy = pltpu.make_async_remote_copy(
            src_ref=source,
            dst_ref=target,
            send_sem=ss.at[phase, 0],
            recv_sem=rs.at[phase, n - 1],
            device_id=(ep, partner),
            device_id_type=MESH,
        )
        copy.start()
        outgoing.append(copy)
        return copy

    def along_z(phase, source, recv):
        def descriptor(a, slot):
            return pltpu.make_async_remote_copy(
                src_ref=source(lax.rem(chip + a, chips)),
                dst_ref=recv.at[slot],
                send_sem=ss.at[phase, a],
                recv_sem=rs.at[phase, slot],
                device_id=(ep, z_peer(a)),
                device_id_type=MESH,
            )

        for a in z_order:
            copy = descriptor(a, chip)
            copy.start()
            outgoing.append(copy)

        def wait():
            for a in reversed(z_order):
                descriptor(a, lax.rem(chip + a, chips)).wait_recv()

        return wait

    a_start, a_arrived, a_sent = exchange(0, send_a, recv_a)
    b_start, b_arrived, b_sent = exchange(1, send_b, recv_b)
    e_start, e_arrived, e_sent = exchange(3, send_e, recv_e, 6)
    h_start, h_arrived, h_sent = exchange(7, send_h, recv_h, 4)
    recv_h[...] = jnp.zeros_like(recv_h)

    copies["tokens"].wait()
    copies["attn_gain"].wait()
    x = tokens[...].astype(F32)
    normed = x * lax.rsqrt(jnp.mean(x * x, axis=-1, keepdims=True) + EPS) * attn_gain[...]
    normed = normed.astype(BF16)
    for i in range(n):
        send_a[i] = normed[:, i * cols : (i + 1) * cols]
    recv_a[ep] = send_a[ep]
    pl.semaphore_wait(barrier, n - 1 + chips)
    a_start(ep_peers)
    for name in late:
        copies[name].start()

    for name in ("lengths", "groups", "members", "gates", "logits"):
        copies[name].wait()
    rows_s[...] = jnp.zeros_like(rows_s)
    rows_s[0:1, 0:seqs] = lengths_ref[...].astype(F32)
    rows_s[1:2, 0:seqs] = groups_ref[...].astype(F32)
    rows_s[2:4, 0:seqs] = members_ref[...].astype(F32)
    rows_s[4:5, 0:seqs] = gates_ref[...]
    rows_s[5:7, 0:seqs] = logits_ref[...]
    rows = rows_s[...][:, 0:seqs]
    eye = (iota((seqs, seqs), 0) == iota((seqs, seqs), 1)).astype(F32)
    columns = exact_dot(eye, rows, NT)
    id0_row = rows[1:2] * EPG + rows[2:3]
    id1_row = rows[1:2] * EPG + rows[3:4]
    id0_col = columns[:, 1:2] * EPG + columns[:, 2:3]
    id1_col = columns[:, 1:2] * EPG + columns[:, 3:4]
    logit_max = jnp.maximum(columns[:, 5:6], columns[:, 6:7])
    exp0 = jnp.exp(columns[:, 5:6] - logit_max)
    exp1 = jnp.exp(columns[:, 6:7] - logit_max)
    exp_sum = exp0 + exp1
    share0 = exp0 / exp_sum * columns[:, 4:5]
    share1 = exp1 / exp_sum * columns[:, 4:5]
    tall = 8 * n
    tall_row = iota((tall, seqs), 0)
    tall_expert = (tall_row // 8).astype(F32)
    tall_kind = tall_row % 8
    tall_rank = jnp.where((tall_kind == 2) | (tall_kind == 3) | (tall_kind == 5), 1.0, 0.0)
    chosen = ((id0_row == tall_expert) | (id1_row == tall_expert)).astype(F32)
    before = (iota((seqs, seqs), 0) < iota((seqs, seqs), 1)).astype(F32)
    rank = exact_dot(chosen, before)
    dispatch = jnp.where((rank == tall_rank) & (tall_kind < 6), chosen, 0.0)
    first = (tall_kind == 0) | (tall_kind == 2)
    second = (tall_kind == 1) | (tall_kind == 3)
    kinds = [jnp.where(kind, dispatch, 0.0) for kind in (first, second, tall_kind >= 4)]
    routes = jnp.concatenate(kinds * 3, axis=1).astype(BF16)
    wide_col = iota((seqs, tall), 1)
    wide_expert = (wide_col // 8).astype(F32)
    wide_kind = wide_col % 8
    wide_rank = jnp.where(wide_kind >= 2, 1.0, 0.0)
    hit0 = (id0_col == wide_expert).astype(F32)
    hit1 = (id1_col == wide_expert).astype(F32)
    after = (iota((seqs, seqs), 1) < iota((seqs, seqs), 0)).astype(F32)
    wide_ranks = exact_dot(after, hit0 + hit1)
    combine = jnp.where((wide_ranks == wide_rank) & (wide_kind < 4), hit0 * share0 + hit1 * share1, 0.0)

    parts = []
    for h in range(2):
        rest = jnp.where(wide_kind % 2 == h, combine, 0.0)
        for _ in range(3):
            part = rest.astype(BF16)
            parts.append(part)
            rest = rest - part.astype(F32)
    shares = jnp.concatenate(parts, axis=0)

    for name in ("wq", "wk", "wv"):
        copies[name].wait()
    wait_all(a_arrived)
    everyone = recv_a[...].reshape(n * seqs, cols)
    partial = jnp.dot(everyone, wqkv[...], preferred_element_type=F32)
    send_b[...] = partial.reshape(n, seqs, 3 * hd)
    b_start(ep_peers)
    recv_b[ep] = send_b[ep]
    wait_all(b_arrived)
    projected = jnp.sum(recv_b[...], axis=0).astype(BF16)
    query = projected[:, 0:hd]
    fresh_k = projected[:, hd : 2 * hd]
    fresh_v = projected[:, 2 * hd : 3 * hd]
    out_ref[:, cols:] = projected[:, hd:]

    total_heads = n
    slope = jnp.float32(0.0)
    for h in range(total_heads):
        slope = jnp.where(tp == h, jnp.float32(2.0 ** (-8.0 * (h + 1.0) / total_heads)), slope)
    scale = half ** (-0.5)
    some = seqs // 2
    both = 2 * some
    q_all = query.astype(F32)
    k_all = fresh_k.astype(F32)
    v_all = fresh_v.astype(F32)
    own_map = (iota((both, hd), 0) // some) == (iota((both, hd), 1) // half)
    q4_seq = iota((both, 2 * hd), 0) % some
    q4_side = iota((both, 2 * hd), 1) // hd
    place = iota((both, cache), 1).astype(F32)
    mix_seq = iota((some, hd), 0)
    copies["keys"].wait()
    scores = []
    for part in range(2):
        at = slice(part * some, (part + 1) * some)
        q2 = jnp.where(own_map, jnp.concatenate([q_all[at], q_all[at]], axis=0), 0.0)
        q4 = jnp.concatenate([q2, q2], axis=1)
        old = jnp.zeros((both, cache), F32)
        for p in range(some // 2):
            lhs = jnp.where(q4_seq == 2 * p + q4_side, q4, 0.0).astype(BF16)
            b0 = part * some + 2 * p
            rhs = jnp.concatenate([keys[b0], keys[b0 + 1]], axis=1)
            old = old + lax.dot_general(lhs, rhs, NT, preferred_element_type=F32)
        scores.append((q2, old * scale))
    copies["vals"].wait()
    lam = lam_h[0]
    mixes = []
    for part, (q2, old) in enumerate(scores):
        at = slice(part * some, (part + 1) * some)
        new = jnp.sum(q2 * jnp.concatenate([k_all[at], k_all[at]], axis=0), axis=-1, keepdims=True) * scale
        count = jnp.concatenate([columns[at, 0:1], columns[at, 0:1]], axis=0)
        old = jnp.where(place < count, old - slope * (count - place), -jnp.inf)
        top = jnp.maximum(jnp.max(old, axis=-1, keepdims=True), new)
        e_old = jnp.exp(old - top)
        e_new = jnp.exp(new - top)
        norm = jnp.sum(e_old, axis=-1, keepdims=True) + e_new
        m_old = e_old / norm
        m_new = e_new / norm
        weights = (m_old[:some] - lam * m_old[some:]).astype(BF16)
        w_new = (m_new[:some] - lam * m_new[some:]).astype(BF16).astype(F32)
        mix = w_new * v_all[at]
        for p in range(some // 2):
            b0 = part * some + 2 * p
            pair = jnp.concatenate([vals[b0], vals[b0 + 1]], axis=1)
            both_mix = jnp.dot(weights, pair, preferred_element_type=F32)
            mix = mix + jnp.where(mix_seq == 2 * p, both_mix[:, :hd], 0.0)
            mix = mix + jnp.where(mix_seq == 2 * p + 1, both_mix[:, hd:], 0.0)
        mixes.append(mix)
    head_mix = jnp.concatenate(mixes, axis=0)
    copies["head_gain"].wait()
    head_out = head_mix * lax.rsqrt(jnp.mean(head_mix * head_mix, axis=-1, keepdims=True) + EPS)
    head_out = (head_out * head_gain[...]).astype(BF16)

    copies["wo"].wait()

    def term_block(z, c):
        at = pl.ds(pl.multiple_of((2 * z + c) * cols, cols), cols)
        return jnp.dot(head_out, wo[:, at], preferred_element_type=F32).astype(BF16)

    for z in range(chips):
        term_out[z] = term_block(z, 1 - core)
    term_copy = to_partner(2, term_out, term_in)
    for z in range(chips):
        term_own[z] = term_block(z, core).astype(F32)
    term_copy.wait_recv()
    send_c[...] = (term_own[...] + term_in[...].astype(F32)).astype(BF16)
    c_wait = along_z(2, lambda i: send_c.at[i], recv_c)
    recv_c[chip] = send_c[chip]
    c_wait()
    attn_sum = jnp.sum(recv_c[...].astype(F32), axis=0)
    own_cols = pl.ds(pl.multiple_of(tp * cols, cols), cols)
    resid = tokens[:, own_cols].astype(F32) + attn_sum

    squares = jnp.broadcast_to(jnp.sum(resid * resid, axis=-1, keepdims=True), (seqs, 128))
    rest = [resid[:, :128], resid[:, 128:], squares]
    parts = []
    for _ in range(3):
        part = [r.astype(BF16) for r in rest]
        rest = [r - p.astype(F32) for r, p in zip(rest, part)]
        parts += part
    packed = jnp.dot(routes, jnp.concatenate(parts, axis=0), preferred_element_type=F32)
    send_e[...] = packed
    recv_e[pl.ds(pl.multiple_of(ep * 8, 8), 8), :] = send_e[pl.ds(pl.multiple_of(ep * 8, 8), 8), :]

    e_start(ep_peers)
    wait_all(e_arrived)

    def tile_row(ref, j):
        return ref[pl.ds(j, n, stride=8), :]

    token_rows = [
        jnp.concatenate([tile_row(recv_e, 2 * r), tile_row(recv_e, 2 * r + 1)], axis=1) for r in range(2)
    ]
    slab = jnp.concatenate(token_rows, axis=0)
    copies["moe_gain"].wait()
    send_f[...] = (slab * moe_gain[:, own_cols]).astype(BF16)
    on_lane = iota((n, 128), 0) == iota((n, 128), 1)
    on_next = iota((n, 128), 0) + n == iota((n, 128), 1)
    stat = jnp.where(on_lane, tile_row(recv_e, 4), 0.0) + jnp.where(on_next, tile_row(recv_e, 5), 0.0)
    send_s[...] = jnp.sum(stat, axis=0, keepdims=True)
    recv_f[tp] = send_f[...]

    recv_s[chip] = send_s[...]
    s_wait = along_z(5, lambda i: send_s, recv_s)

    def row_copy(source, slot, target, lane):
        return pltpu.make_async_remote_copy(
            src_ref=source,
            dst_ref=recv_f.at[slot],
            send_sem=ss.at[4, lane],
            recv_sem=rs.at[4, slot],
            device_id=(ep, target),
            device_id_type=MESH,
        )

    rows_out = [row_copy(send_f, tp, z_peer(a), a) for a in z_order]
    rows_out.append(row_copy(send_f, tp, partner, 0))
    for copy in rows_out:
        copy.start()
    for a in reversed(z_order):
        slot = z_peer(a)
        row_copy(send_f, slot, slot, a).wait_recv()
        copy = row_copy(recv_f.at[slot], slot, partner, chips + a)
        copy.start()
        rows_out.append(copy)
    outgoing.extend(rows_out)
    for name in ("wg", "wu"):
        copies[name].wait()
    slots = 2 * n
    s_wait()
    pair_s[...] = jnp.sum(recv_s[...], axis=0)
    stat_copy = to_partner(5, pair_s, stat_in)
    for a in range(chips):
        slot = lax.rem(chip + a, chips) * 2 + 1 - core
        row_copy(send_f, slot, partner, a).wait_recv()
    everything = jnp.concatenate([recv_f[i] for i in range(n)], axis=1)
    gate_up = jnp.dot(everything, wgu[...], preferred_element_type=F32)
    stat_copy.wait_recv()
    stats = jnp.broadcast_to(pair_s[...] + stat_in[...], (8, 128))
    eye_slots = (iota((slots, 128), 0) == iota((slots, 128), 1)).astype(F32)
    sums = exact_dot(eye_slots, stats, NT)[:, 0:1]
    norm_scale = lax.rsqrt(sums / width + EPS)
    gate = gate_up[:, :hd] * norm_scale
    upper = gate_up[:, hd:] * norm_scale
    hidden = (gate / (1.0 + jnp.exp(-gate)) * upper).astype(BF16)

    copies["wd"].wait()

    def down_block(z, c):
        at = pl.ds(pl.multiple_of((2 * z + c) * cols, cols), cols)
        return jnp.dot(hidden, wd[:, at], preferred_element_type=F32)

    for z in range(chips):
        pair_out[z] = down_block(z, 1 - core).astype(BF16)
    pair_copy = to_partner(6, pair_out, pair_in)
    for z in range(chips):
        pair_own[z] = down_block(z, core)
    pair_copy.wait_recv()
    send_g[...] = (pair_own[...] + pair_in[...].astype(F32)).astype(BF16)
    g_wait = along_z(6, lambda i: send_g.at[i], recv_g)
    recv_g[chip] = send_g[chip]
    g_wait()
    expert_out = jnp.sum(recv_g[...].astype(F32), axis=0).astype(BF16).astype(F32)

    for r in range(2):
        for h in range(2):
            send_h[pl.ds(2 * r + h, n, stride=8), :] = expert_out[r * n : (r + 1) * n, h * 128 : (h + 1) * 128]
    recv_h[pl.ds(pl.multiple_of(ep * 8, 8), 4), :] = send_h[pl.ds(pl.multiple_of(ep * 8, 8), 4), :]
    h_start(ep_peers)
    for sent in (a_sent, b_sent, e_sent, h_sent):
        lax.fori_loop(1, n, sent, 0)
    for copy in outgoing:
        copy.wait_send()
    wait_all(h_arrived)
    back = jnp.dot(shares, recv_h[...].astype(BF16), preferred_element_type=F32)
    routed = [sum(back[(3 * h + i) * seqs : (3 * h + i + 1) * seqs] for i in range(3)) for h in range(2)]
    out_ref[:, :cols] = (resid + jnp.concatenate(routed, axis=1)).astype(BF16)


def unpack_kernel(packed_ref, mixed_ref, fresh_k_ref, fresh_v_ref, sems):
    copies = []
    at = 0
    for i, ref in enumerate((mixed_ref, fresh_k_ref, fresh_v_ref)):
        size = ref.shape[1]
        copies.append(pltpu.make_async_copy(packed_ref.at[:, pl.ds(at, size)], ref, sems.at[i]))
        at += size
    for copy in copies:
        copy.start()
    for copy in copies:
        copy.wait()


def on_device(n, *args):
    (tokens, attn_gain, w_query, w_key, w_value, mix_lambda, head_gain, w_output, cache_keys, cache_value) = args[:10]
    (lengths, moe_gain, group_ids, member_ids, group_gate, member_logits, w_exp_gate, w_exp_up, w_exp_down) = args[10:]
    seqs, width = tokens.shape
    cols = width // n
    hd = w_query.shape[1]
    cache = cache_keys.shape[1]
    operands = (
        tokens,
        attn_gain.reshape(1, width),
        w_query,
        w_key,
        w_value,
        mix_lambda,
        head_gain.reshape(1, hd),
        w_output,
        cache_keys,
        cache_value,
        lengths.reshape(1, seqs),
        moe_gain.reshape(1, width),
        group_ids.reshape(1, seqs),
        member_ids.T,
        group_gate.reshape(1, seqs),
        member_logits.T,
        w_exp_gate,
        w_exp_up,
        w_exp_down,
    )
    vmem = pl.BlockSpec(memory_space=pltpu.VMEM)
    hbm = pl.BlockSpec(memory_space=pl.ANY)
    scratch = [
        pltpu.VMEM((seqs, width), BF16),
        pltpu.VMEM((1, width), F32),
        pltpu.VMEM((w_query.shape[0], 3 * hd), BF16),
        pltpu.SMEM((1,), F32),
        pltpu.VMEM((1, seqs), jnp.int32),
        pltpu.VMEM((1, seqs), jnp.int32),
        pltpu.VMEM((2, seqs), jnp.int32),
        pltpu.VMEM((1, seqs), F32),
        pltpu.VMEM((2, seqs), F32),
        pltpu.VMEM((1, hd), F32),
        pltpu.VMEM((hd, width), BF16),
        pltpu.VMEM((seqs, cache, hd), BF16),
        pltpu.VMEM((seqs, cache, hd), BF16),
        pltpu.VMEM((1, width), F32),
        pltpu.VMEM((width, 2 * hd), BF16),
        pltpu.VMEM((hd, width), BF16),
        pltpu.VMEM((8, 128), F32),
        pltpu.VMEM((n, seqs, cols), BF16),
        pltpu.VMEM((n, seqs, cols), BF16),
        pltpu.VMEM((n, seqs, 3 * hd), F32),
        pltpu.VMEM((n, seqs, 3 * hd), F32),
        pltpu.VMEM((n // 2, seqs, cols), BF16),
        pltpu.VMEM((n // 2, seqs, cols), BF16),
        pltpu.VMEM((n // 2, seqs, cols), F32),
        pltpu.VMEM((n // 2, seqs, cols), BF16),
        pltpu.VMEM((n // 2, seqs, cols), BF16),
        pltpu.VMEM((8 * n, 128), F32),
        pltpu.VMEM((8 * n, 128), F32),
        pltpu.VMEM((2 * n, cols), BF16),
        pltpu.VMEM((n, 2 * n, cols), BF16),
        pltpu.VMEM((1, 128), F32),
        pltpu.VMEM((1, 128), F32),
        pltpu.VMEM((1, 128), F32),
        pltpu.VMEM((n // 2, 1, 128), F32),
        pltpu.VMEM((n // 2, 2 * n, cols), BF16),
        pltpu.VMEM((n // 2, 2 * n, cols), BF16),
        pltpu.VMEM((n // 2, 2 * n, cols), F32),
        pltpu.VMEM((n // 2, 2 * n, cols), BF16),
        pltpu.VMEM((n // 2, 2 * n, cols), BF16),
        pltpu.VMEM((8 * n, 128), F32),
        pltpu.VMEM((8 * n, 128), F32),
        pltpu.SemaphoreType.DMA((19,)),
        pltpu.SemaphoreType.DMA((8, n)),
        pltpu.SemaphoreType.DMA((8, n)),
    ]
    packed = pl.pallas_call(
        functools.partial(layer_kernel, n),
        out_shape=pltpu.VMEM((seqs, cols + 2 * hd), BF16),
        in_specs=[pl.BlockSpec(memory_space=pltpu.SMEM) if i == 5 else hbm for i in range(len(operands))],
        out_specs=vmem,
        scratch_shapes=scratch,
        compiler_params=pltpu.CompilerParams(collective_id=0, has_side_effects=True),
        name="layer",
    )(*operands)
    return pl.pallas_call(
        unpack_kernel,
        out_shape=(
            jax.ShapeDtypeStruct((seqs, cols), BF16),
            jax.ShapeDtypeStruct((seqs, hd), BF16),
            jax.ShapeDtypeStruct((seqs, hd), BF16),
        ),
        in_specs=[vmem],
        out_specs=(hbm, hbm, hbm),
        scratch_shapes=[pltpu.SemaphoreType.DMA((3,))],
        name="unpack",
    )(pltpu.with_memory_space_constraint(packed, pltpu.VMEM))


def solution(mesh):
    n = mesh.shape["ep"]
    return jax.shard_map(
        functools.partial(on_device, n),
        mesh=mesh,
        in_specs=(
            P("ep", None),
            P(),
            P("ep", "tp"),
            P("ep", "tp"),
            P("ep", "tp"),
            P("tp"),
            P(),
            P("tp", None),
            P("ep", None, "tp"),
            P("ep", None, "tp"),
            P("ep"),
            P(),
            P("ep"),
            P("ep", None),
            P("ep"),
            P("ep", None),
            P("ep", None, "tp"),
            P("ep", None, "tp"),
            P("ep", "tp", None),
        ),
        out_specs=(P("ep", "tp"), P("ep", "tp"), P("ep", "tp")),
        check_vma=False,
    )
```

```python
import functools

import jax
import jax.numpy as jnp
from jax import lax
from jax.experimental import pallas as pl
from jax.experimental.pallas import tpu as pltpu
from jax.sharding import PartitionSpec as P

EPG = 2
EPS = 1e-06
MESH = pl.DeviceIdType.MESH
HIGHEST = lax.Precision.HIGHEST
F32 = jnp.float32
BF16 = jnp.bfloat16
NT = (((1,), (1,)), ((), ()))


def iota(shape, dim):
    return lax.broadcasted_iota(jnp.int32, shape, dim)


def exact_dot(a, b, dims=(((1,), (0,)), ((), ()))):
    return lax.dot_general(a, b, dims, precision=HIGHEST, preferred_element_type=F32)


def layer_kernel(
    n,
    tokens_h,
    attn_gain_h,
    wq_h,
    wk_h,
    wv_h,
    lam_h,
    head_gain_h,
    wo_h,
    keys_h,
    vals_h,
    lengths_h,
    moe_gain_h,
    groups_h,
    members_h,
    gates_h,
    logits_h,
    wg_h,
    wu_h,
    wd_h,
    out_ref,
    tokens,
    attn_gain,
    wqkv,
    lam_ref,
    lengths_ref,
    groups_ref,
    members_ref,
    gates_ref,
    logits_ref,
    head_gain,
    wo,
    keys,
    vals,
    moe_gain,
    wgu,
    wd,
    rows_s,
    send_a,
    recv_a,
    send_b,
    recv_b,
    term_out,
    term_in,
    term_own,
    send_c,
    recv_c,
    send_e,
    recv_e,
    send_f,
    recv_f,
    send_s,
    stat_in,
    pair_s,
    recv_s,
    pair_out,
    pair_in,
    pair_own,
    send_g,
    recv_g,
    send_h,
    recv_h,
    load_sem,
    ss,
    rs,
):
    ep = lax.axis_index("ep")
    tp = lax.axis_index("tp")
    core = lax.rem(tp, 2)
    partner = tp + 1 - 2 * core
    chips = n // 2
    chip = tp // 2
    width = tokens_h.shape[1]
    cols = width // n
    seqs = tokens_h.shape[0]
    hd = wq_h.shape[1]
    half = hd // 2
    cache = keys_h.shape[1]

    side = 4
    ep_offsets = [(a, b) for a in range(side) for b in range(n // side) if (a, b) != (0, 0)]

    def ep_hops(o):
        return min(o[0], side - o[0]) + min(o[1], n // side - o[1])

    def ep_peer(o):
        return lax.rem(ep // side + o[0], side) * side + lax.rem(ep % side + o[1], side)

    ep_offsets.sort(key=lambda o: -ep_hops(o))
    ep_peers = [ep_peer(o) for o in ep_offsets]
    z_order = sorted(range(1, chips), key=lambda a: -min(a, chips - a))

    def z_peer(a):
        return lax.rem(chip + a, chips) * 2 + core

    loads = {
        "tokens": (tokens_h, tokens),
        "attn_gain": (attn_gain_h, attn_gain),
        "wq": (wq_h, wqkv.at[:, pl.ds(0, hd)]),
        "wk": (wk_h, wqkv.at[:, pl.ds(hd, hd)]),
        "wv": (wv_h, wqkv.at[:, pl.ds(2 * hd, hd)]),
        "lengths": (lengths_h, lengths_ref),
        "groups": (groups_h, groups_ref),
        "members": (members_h, members_ref),
        "gates": (gates_h, gates_ref),
        "logits": (logits_h, logits_ref),
        "head_gain": (head_gain_h, head_gain),
        "moe_gain": (moe_gain_h, moe_gain),
        "keys": (keys_h, keys),
        "vals": (vals_h, vals),
        "wo": (wo_h, wo),
        "wg": (wg_h.at[0], wgu.at[:, pl.ds(0, hd)]),
        "wu": (wu_h.at[0], wgu.at[:, pl.ds(hd, hd)]),
        "wd": (wd_h.at[0], wd),
    }
    copies = {
        name: pltpu.make_async_copy(source, target, load_sem.at[i])
        for i, (name, (source, target)) in enumerate(loads.items())
    }
    copies["tokens"].start()
    copies["attn_gain"].start()

    barrier = pltpu.get_barrier_semaphore()
    for peer in ep_peers:
        pl.semaphore_signal(barrier, inc=1, device_id=(peer, tp), device_id_type=MESH)
    for a in z_order:
        pl.semaphore_signal(barrier, inc=1, device_id=(ep, z_peer(a)), device_id_type=MESH)
    pl.semaphore_signal(barrier, inc=1, device_id=(ep, partner), device_id_type=MESH)

    late = ("keys", "vals", "wo", "wg", "wu", "wd")
    for name, copy in copies.items():
        if name not in late + ("tokens", "attn_gain"):
            copy.start()

    def exchange(phase, send, recv, tile_rows=None):
        def block(ref, i):
            return ref.at[i] if tile_rows is None else ref.at[pl.ds(pl.multiple_of(i * 8, 8), tile_rows), :]

        def descriptor(peer, incoming):
            return pltpu.make_async_remote_copy(
                src_ref=block(send, peer),
                dst_ref=block(recv, peer if incoming else ep),
                send_sem=ss.at[phase, peer],
                recv_sem=rs.at[phase, peer if incoming else ep],
                device_id=(peer, tp),
                device_id_type=MESH,
            )

        def start(peers):
            for peer in peers:
                descriptor(peer, False).start()

        def arrived(peer):
            descriptor(peer, True).wait_recv()

        def sent(d, carry):
            descriptor(lax.rem(ep + d, n), False).wait_send()
            return carry

        return start, arrived, sent

    def wait_all(arrived):
        def body(d, carry):
            arrived(lax.rem(ep + d, n))
            return carry

        lax.fori_loop(1, n, body, 0)

    outgoing = []

    def to_partner(phase, source, target):
        copy = pltpu.make_async_remote_copy(
            src_ref=source,
            dst_ref=target,
            send_sem=ss.at[phase, 0],
            recv_sem=rs.at[phase, n - 1],
            device_id=(ep, partner),
            device_id_type=MESH,
        )
        copy.start()
        outgoing.append(copy)
        return copy

    def along_z(phase, source, recv):
        def descriptor(a, slot):
            return pltpu.make_async_remote_copy(
                src_ref=source(lax.rem(chip + a, chips)),
                dst_ref=recv.at[slot],
                send_sem=ss.at[phase, a],
                recv_sem=rs.at[phase, slot],
                device_id=(ep, z_peer(a)),
                device_id_type=MESH,
            )

        for a in z_order:
            copy = descriptor(a, chip)
            copy.start()
            outgoing.append(copy)

        def wait():
            for a in reversed(z_order):
                descriptor(a, lax.rem(chip + a, chips)).wait_recv()

        return wait

    a_start, a_arrived, a_sent = exchange(0, send_a, recv_a)
    b_start, b_arrived, b_sent = exchange(1, send_b, recv_b)
    e_start, e_arrived, e_sent = exchange(3, send_e, recv_e, 6)
    h_start, h_arrived, h_sent = exchange(7, send_h, recv_h, 4)
    recv_h[...] = jnp.zeros_like(recv_h)

    copies["tokens"].wait()
    copies["attn_gain"].wait()
    x = tokens[...].astype(F32)
    normed = x * lax.rsqrt(jnp.mean(x * x, axis=-1, keepdims=True) + EPS) * attn_gain[...]
    normed = normed.astype(BF16)
    for i in range(n):
        send_a[i] = normed[:, i * cols : (i + 1) * cols]
    recv_a[ep] = send_a[ep]
    pl.semaphore_wait(barrier, n - 1 + chips)
    a_start(ep_peers)
    for name in late:
        copies[name].start()

    for name in ("lengths", "groups", "members", "gates", "logits"):
        copies[name].wait()
    rows_s[...] = jnp.zeros_like(rows_s)
    rows_s[0:1, 0:seqs] = lengths_ref[...].astype(F32)
    rows_s[1:2, 0:seqs] = groups_ref[...].astype(F32)
    rows_s[2:4, 0:seqs] = members_ref[...].astype(F32)
    rows_s[4:5, 0:seqs] = gates_ref[...]
    rows_s[5:7, 0:seqs] = logits_ref[...]
    rows = rows_s[...][:, 0:seqs]
    eye = (iota((seqs, seqs), 0) == iota((seqs, seqs), 1)).astype(F32)
    columns = exact_dot(eye, rows, NT)
    id0_row = rows[1:2] * EPG + rows[2:3]
    id1_row = rows[1:2] * EPG + rows[3:4]
    id0_col = columns[:, 1:2] * EPG + columns[:, 2:3]
    id1_col = columns[:, 1:2] * EPG + columns[:, 3:4]
    logit_max = jnp.maximum(columns[:, 5:6], columns[:, 6:7])
    exp0 = jnp.exp(columns[:, 5:6] - logit_max)
    exp1 = jnp.exp(columns[:, 6:7] - logit_max)
    exp_sum = exp0 + exp1
    share0 = exp0 / exp_sum * columns[:, 4:5]
    share1 = exp1 / exp_sum * columns[:, 4:5]
    tall = 8 * n
    tall_row = iota((tall, seqs), 0)
    tall_expert = (tall_row // 8).astype(F32)
    tall_kind = tall_row % 8
    tall_rank = jnp.where((tall_kind == 2) | (tall_kind == 3) | (tall_kind == 5), 1.0, 0.0)
    chosen = ((id0_row == tall_expert) | (id1_row == tall_expert)).astype(F32)
    before = (iota((seqs, seqs), 0) < iota((seqs, seqs), 1)).astype(F32)
    rank = exact_dot(chosen, before)
    dispatch = jnp.where((rank == tall_rank) & (tall_kind < 6), chosen, 0.0)
    first = (tall_kind == 0) | (tall_kind == 2)
    second = (tall_kind == 1) | (tall_kind == 3)
    kinds = [jnp.where(kind, dispatch, 0.0) for kind in (first, second, tall_kind >= 4)]
    routes = jnp.concatenate(kinds * 3, axis=1).astype(BF16)
    wide_col = iota((seqs, tall), 1)
    wide_expert = (wide_col // 8).astype(F32)
    wide_kind = wide_col % 8
    wide_rank = jnp.where(wide_kind >= 2, 1.0, 0.0)
    hit0 = (id0_col == wide_expert).astype(F32)
    hit1 = (id1_col == wide_expert).astype(F32)
    after = (iota((seqs, seqs), 1) < iota((seqs, seqs), 0)).astype(F32)
    wide_ranks = exact_dot(after, hit0 + hit1)
    combine = jnp.where((wide_ranks == wide_rank) & (wide_kind < 4), hit0 * share0 + hit1 * share1, 0.0)

    parts = []
    for h in range(2):
        rest = jnp.where(wide_kind % 2 == h, combine, 0.0)
        for _ in range(3):
            part = rest.astype(BF16)
            parts.append(part)
            rest = rest - part.astype(F32)
    shares = jnp.concatenate(parts, axis=0)

    for name in ("wq", "wk", "wv"):
        copies[name].wait()
    wait_all(a_arrived)
    everyone = recv_a[...].reshape(n * seqs, cols)
    partial = jnp.dot(everyone, wqkv[...], preferred_element_type=F32)
    send_b[...] = partial.reshape(n, seqs, 3 * hd)
    b_start(ep_peers)
    recv_b[ep] = send_b[ep]
    wait_all(b_arrived)
    projected = jnp.sum(recv_b[...], axis=0).astype(BF16)
    query = projected[:, 0:hd]
    fresh_k = projected[:, hd : 2 * hd]
    fresh_v = projected[:, 2 * hd : 3 * hd]
    out_ref[:, cols:] = projected[:, hd:]

    total_heads = n
    slope = jnp.float32(0.0)
    for h in range(total_heads):
        slope = jnp.where(tp == h, jnp.float32(2.0 ** (-8.0 * (h + 1.0) / total_heads)), slope)
    scale = half ** (-0.5)
    some = seqs // 2
    both = 2 * some
    q_all = query.astype(F32)
    k_all = fresh_k.astype(F32)
    v_all = fresh_v.astype(F32)
    own_map = (iota((both, hd), 0) // some) == (iota((both, hd), 1) // half)
    q4_seq = iota((both, 2 * hd), 0) % some
    q4_side = iota((both, 2 * hd), 1) // hd
    place = iota((both, cache), 1).astype(F32)
    mix_seq = iota((some, hd), 0)
    copies["keys"].wait()
    scores = []
    for part in range(2):
        at = slice(part * some, (part + 1) * some)
        q2 = jnp.where(own_map, jnp.concatenate([q_all[at], q_all[at]], axis=0), 0.0)
        q4 = jnp.concatenate([q2, q2], axis=1)
        old = jnp.zeros((both, cache), F32)
        for p in range(some // 2):
            lhs = jnp.where(q4_seq == 2 * p + q4_side, q4, 0.0).astype(BF16)
            b0 = part * some + 2 * p
            rhs = jnp.concatenate([keys[b0], keys[b0 + 1]], axis=1)
            old = old + lax.dot_general(lhs, rhs, NT, preferred_element_type=F32)
        scores.append((q2, old * scale))
    copies["vals"].wait()
    lam = lam_h[0]
    mixes = []
    for part, (q2, old) in enumerate(scores):
        at = slice(part * some, (part + 1) * some)
        new = jnp.sum(q2 * jnp.concatenate([k_all[at], k_all[at]], axis=0), axis=-1, keepdims=True) * scale
        count = jnp.concatenate([columns[at, 0:1], columns[at, 0:1]], axis=0)
        old = jnp.where(place < count, old - slope * (count - place), -jnp.inf)
        top = jnp.maximum(jnp.max(old, axis=-1, keepdims=True), new)
        e_old = jnp.exp(old - top)
        e_new = jnp.exp(new - top)
        norm = jnp.sum(e_old, axis=-1, keepdims=True) + e_new
        m_old = e_old / norm
        m_new = e_new / norm
        weights = (m_old[:some] - lam * m_old[some:]).astype(BF16)
        w_new = (m_new[:some] - lam * m_new[some:]).astype(BF16).astype(F32)
        mix = w_new * v_all[at]
        for p in range(some // 2):
            b0 = part * some + 2 * p
            pair = jnp.concatenate([vals[b0], vals[b0 + 1]], axis=1)
            both_mix = jnp.dot(weights, pair, preferred_element_type=F32)
            mix = mix + jnp.where(mix_seq == 2 * p, both_mix[:, :hd], 0.0)
            mix = mix + jnp.where(mix_seq == 2 * p + 1, both_mix[:, hd:], 0.0)
        mixes.append(mix)
    head_mix = jnp.concatenate(mixes, axis=0)
    copies["head_gain"].wait()
    head_out = head_mix * lax.rsqrt(jnp.mean(head_mix * head_mix, axis=-1, keepdims=True) + EPS)
    head_out = (head_out * head_gain[...]).astype(BF16)

    copies["wo"].wait()

    def term_block(z, c):
        at = pl.ds(pl.multiple_of((2 * z + c) * cols, cols), cols)
        return jnp.dot(head_out, wo[:, at], preferred_element_type=F32).astype(BF16)

    for z in range(chips):
        term_out[z] = term_block(z, 1 - core)
    term_copy = to_partner(2, term_out, term_in)
    for z in range(chips):
        term_own[z] = term_block(z, core).astype(F32)
    term_copy.wait_recv()
    send_c[...] = (term_own[...] + term_in[...].astype(F32)).astype(BF16)
    c_wait = along_z(2, lambda i: send_c.at[i], recv_c)
    recv_c[chip] = send_c[chip]
    for sent in (a_sent, b_sent):
        lax.fori_loop(1, n, sent, 0)
    c_wait()
    attn_sum = jnp.sum(recv_c[...].astype(F32), axis=0)
    own_cols = pl.ds(pl.multiple_of(tp * cols, cols), cols)
    resid = tokens[:, own_cols].astype(F32) + attn_sum

    squares = jnp.broadcast_to(jnp.sum(resid * resid, axis=-1, keepdims=True), (seqs, 128))
    rest = [resid[:, :128], resid[:, 128:], squares]
    parts = []
    for _ in range(3):
        part = [r.astype(BF16) for r in rest]
        rest = [r - p.astype(F32) for r, p in zip(rest, part)]
        parts += part
    packed = jnp.dot(routes, jnp.concatenate(parts, axis=0), preferred_element_type=F32)
    send_e[...] = packed
    recv_e[pl.ds(pl.multiple_of(ep * 8, 8), 8), :] = send_e[pl.ds(pl.multiple_of(ep * 8, 8), 8), :]

    e_start(ep_peers)
    wait_all(e_arrived)

    def tile_row(ref, j):
        return ref[pl.ds(j, n, stride=8), :]

    token_rows = [
        jnp.concatenate([tile_row(recv_e, 2 * r), tile_row(recv_e, 2 * r + 1)], axis=1) for r in range(2)
    ]
    slab = jnp.concatenate(token_rows, axis=0)
    copies["moe_gain"].wait()
    send_f[...] = (slab * moe_gain[:, own_cols]).astype(BF16)
    on_lane = iota((n, 128), 0) == iota((n, 128), 1)
    on_next = iota((n, 128), 0) + n == iota((n, 128), 1)
    stat = jnp.where(on_lane, tile_row(recv_e, 4), 0.0) + jnp.where(on_next, tile_row(recv_e, 5), 0.0)
    send_s[...] = jnp.sum(stat, axis=0, keepdims=True)
    recv_f[tp] = send_f[...]

    recv_s[chip] = send_s[...]
    s_wait = along_z(5, lambda i: send_s, recv_s)

    def row_copy(source, slot, target, lane):
        return pltpu.make_async_remote_copy(
            src_ref=source,
            dst_ref=recv_f.at[slot],
            send_sem=ss.at[4, lane],
            recv_sem=rs.at[4, slot],
            device_id=(ep, target),
            device_id_type=MESH,
        )

    rows_out = [row_copy(send_f, tp, z_peer(a), a) for a in z_order]
    rows_out.append(row_copy(send_f, tp, partner, 0))
    for copy in rows_out:
        copy.start()
    for a in reversed(z_order):
        slot = z_peer(a)
        row_copy(send_f, slot, slot, a).wait_recv()
        copy = row_copy(recv_f.at[slot], slot, partner, chips + a)
        copy.start()
        rows_out.append(copy)
    outgoing.extend(rows_out)
    for name in ("wg", "wu"):
        copies[name].wait()
    slots = 2 * n
    s_wait()
    pair_s[...] = jnp.sum(recv_s[...], axis=0)
    stat_copy = to_partner(5, pair_s, stat_in)
    for a in range(chips):
        slot = lax.rem(chip + a, chips) * 2 + 1 - core
        row_copy(send_f, slot, partner, a).wait_recv()
    everything = jnp.concatenate([recv_f[i] for i in range(n)], axis=1)
    gate_up = jnp.dot(everything, wgu[...], preferred_element_type=F32)
    stat_copy.wait_recv()
    stats = jnp.broadcast_to(pair_s[...] + stat_in[...], (8, 128))
    eye_slots = (iota((slots, 128), 0) == iota((slots, 128), 1)).astype(F32)
    sums = exact_dot(eye_slots, stats, NT)[:, 0:1]
    norm_scale = lax.rsqrt(sums / width + EPS)
    gate = gate_up[:, :hd] * norm_scale
    upper = gate_up[:, hd:] * norm_scale
    hidden = (gate / (1.0 + jnp.exp(-gate)) * upper).astype(BF16)

    copies["wd"].wait()

    def down_block(z, c):
        at = pl.ds(pl.multiple_of((2 * z + c) * cols, cols), cols)
        return jnp.dot(hidden, wd[:, at], preferred_element_type=F32)

    for z in range(chips):
        pair_out[z] = down_block(z, 1 - core).astype(BF16)
    pair_copy = to_partner(6, pair_out, pair_in)
    for z in range(chips):
        pair_own[z] = down_block(z, core)
    pair_copy.wait_recv()
    send_g[...] = (pair_own[...] + pair_in[...].astype(F32)).astype(BF16)
    g_wait = along_z(6, lambda i: send_g.at[i], recv_g)
    recv_g[chip] = send_g[chip]
    g_wait()
    expert_out = jnp.sum(recv_g[...].astype(F32), axis=0).astype(BF16).astype(F32)

    for r in range(2):
        for h in range(2):
            send_h[pl.ds(2 * r + h, n, stride=8), :] = expert_out[r * n : (r + 1) * n, h * 128 : (h + 1) * 128]
    recv_h[pl.ds(pl.multiple_of(ep * 8, 8), 4), :] = send_h[pl.ds(pl.multiple_of(ep * 8, 8), 4), :]
    h_start(ep_peers)
    for sent in (e_sent, h_sent):
        lax.fori_loop(1, n, sent, 0)
    for copy in outgoing:
        copy.wait_send()
    wait_all(h_arrived)
    back = jnp.dot(shares, recv_h[...].astype(BF16), preferred_element_type=F32)
    routed = [sum(back[(3 * h + i) * seqs : (3 * h + i + 1) * seqs] for i in range(3)) for h in range(2)]
    out_ref[:, :cols] = (resid + jnp.concatenate(routed, axis=1)).astype(BF16)


def unpack_kernel(packed_ref, mixed_ref, fresh_k_ref, fresh_v_ref, sems):
    copies = []
    at = 0
    for i, ref in enumerate((mixed_ref, fresh_k_ref, fresh_v_ref)):
        size = ref.shape[1]
        copies.append(pltpu.make_async_copy(packed_ref.at[:, pl.ds(at, size)], ref, sems.at[i]))
        at += size
    for copy in copies:
        copy.start()
    for copy in copies:
        copy.wait()


def on_device(n, *args):
    (tokens, attn_gain, w_query, w_key, w_value, mix_lambda, head_gain, w_output, cache_keys, cache_value) = args[:10]
    (lengths, moe_gain, group_ids, member_ids, group_gate, member_logits, w_exp_gate, w_exp_up, w_exp_down) = args[10:]
    seqs, width = tokens.shape
    cols = width // n
    hd = w_query.shape[1]
    cache = cache_keys.shape[1]
    operands = (
        tokens,
        attn_gain.reshape(1, width),
        w_query,
        w_key,
        w_value,
        mix_lambda,
        head_gain.reshape(1, hd),
        w_output,
        cache_keys,
        cache_value,
        lengths.reshape(1, seqs),
        moe_gain.reshape(1, width),
        group_ids.reshape(1, seqs),
        member_ids.T,
        group_gate.reshape(1, seqs),
        member_logits.T,
        w_exp_gate,
        w_exp_up,
        w_exp_down,
    )
    vmem = pl.BlockSpec(memory_space=pltpu.VMEM)
    hbm = pl.BlockSpec(memory_space=pl.ANY)
    scratch = [
        pltpu.VMEM((seqs, width), BF16),
        pltpu.VMEM((1, width), F32),
        pltpu.VMEM((w_query.shape[0], 3 * hd), BF16),
        pltpu.SMEM((1,), F32),
        pltpu.VMEM((1, seqs), jnp.int32),
        pltpu.VMEM((1, seqs), jnp.int32),
        pltpu.VMEM((2, seqs), jnp.int32),
        pltpu.VMEM((1, seqs), F32),
        pltpu.VMEM((2, seqs), F32),
        pltpu.VMEM((1, hd), F32),
        pltpu.VMEM((hd, width), BF16),
        pltpu.VMEM((seqs, cache, hd), BF16),
        pltpu.VMEM((seqs, cache, hd), BF16),
        pltpu.VMEM((1, width), F32),
        pltpu.VMEM((width, 2 * hd), BF16),
        pltpu.VMEM((hd, width), BF16),
        pltpu.VMEM((8, 128), F32),
        pltpu.VMEM((n, seqs, cols), BF16),
        pltpu.VMEM((n, seqs, cols), BF16),
        pltpu.VMEM((n, seqs, 3 * hd), F32),
        pltpu.VMEM((n, seqs, 3 * hd), F32),
        pltpu.VMEM((n // 2, seqs, cols), BF16),
        pltpu.VMEM((n // 2, seqs, cols), BF16),
        pltpu.VMEM((n // 2, seqs, cols), F32),
        pltpu.VMEM((n // 2, seqs, cols), BF16),
        pltpu.VMEM((n // 2, seqs, cols), BF16),
        pltpu.VMEM((8 * n, 128), F32),
        pltpu.VMEM((8 * n, 128), F32),
        pltpu.VMEM((2 * n, cols), BF16),
        pltpu.VMEM((n, 2 * n, cols), BF16),
        pltpu.VMEM((1, 128), F32),
        pltpu.VMEM((1, 128), F32),
        pltpu.VMEM((1, 128), F32),
        pltpu.VMEM((n // 2, 1, 128), F32),
        pltpu.VMEM((n // 2, 2 * n, cols), BF16),
        pltpu.VMEM((n // 2, 2 * n, cols), BF16),
        pltpu.VMEM((n // 2, 2 * n, cols), F32),
        pltpu.VMEM((n // 2, 2 * n, cols), BF16),
        pltpu.VMEM((n // 2, 2 * n, cols), BF16),
        pltpu.VMEM((8 * n, 128), F32),
        pltpu.VMEM((8 * n, 128), F32),
        pltpu.SemaphoreType.DMA((19,)),
        pltpu.SemaphoreType.DMA((8, n)),
        pltpu.SemaphoreType.DMA((8, n)),
    ]
    packed = pl.pallas_call(
        functools.partial(layer_kernel, n),
        out_shape=pltpu.VMEM((seqs, cols + 2 * hd), BF16),
        in_specs=[pl.BlockSpec(memory_space=pltpu.SMEM) if i == 5 else hbm for i in range(len(operands))],
        out_specs=vmem,
        scratch_shapes=scratch,
        compiler_params=pltpu.CompilerParams(collective_id=0, has_side_effects=True),
        name="layer",
    )(*operands)
    return pl.pallas_call(
        unpack_kernel,
        out_shape=(
            jax.ShapeDtypeStruct((seqs, cols), BF16),
            jax.ShapeDtypeStruct((seqs, hd), BF16),
            jax.ShapeDtypeStruct((seqs, hd), BF16),
        ),
        in_specs=[vmem],
        out_specs=(hbm, hbm, hbm),
        scratch_shapes=[pltpu.SemaphoreType.DMA((3,))],
        name="unpack",
    )(pltpu.with_memory_space_constraint(packed, pltpu.VMEM))


def solution(mesh):
    n = mesh.shape["ep"]
    return jax.shard_map(
        functools.partial(on_device, n),
        mesh=mesh,
        in_specs=(
            P("ep", None),
            P(),
            P("ep", "tp"),
            P("ep", "tp"),
            P("ep", "tp"),
            P("tp"),
            P(),
            P("tp", None),
            P("ep", None, "tp"),
            P("ep", None, "tp"),
            P("ep"),
            P(),
            P("ep"),
            P("ep", None),
            P("ep"),
            P("ep", None),
            P("ep", None, "tp"),
            P("ep", None, "tp"),
            P("ep", "tp", None),
        ),
        out_specs=(P("ep", "tp"), P("ep", "tp"), P("ep", "tp")),
        check_vma=False,
    )
```
